32 devices in a mesh: pp: 4 (over y, x), tp: 8 (over z, core).
Axes of the slice: x: 2, y: 2, z: 4, core: 2. Of those that a mesh axis runs over, the one named last changes fastest.
Arguments:
- entry_stream_rows: bfloat16 [256, 2048], P('pp', 'tp'), may hold values from -21 to 21
- layer_rescale_factor: float32 [4, 2048], P('pp'), may hold values from 0.1 to 1.9
- probe_projection: bfloat16 [4, 2048, 2048], P('pp', 'tp'), may hold values from -0.125 to 0.125
- retention_projection: bfloat16 [4, 2048, 2048], P('pp', 'tp'), may hold values from -0.125 to 0.125
- candidate_projection: bfloat16 [4, 2048, 2048], P('pp', 'tp'), may hold values from -0.125 to 0.125
- emission_filter_matrix: bfloat16 [4, 2048, 2048], P('pp', 'tp'), may hold values from -0.125 to 0.125
- retention_minimum: float32 [4, 2048], P('pp', 'tp'), may hold values from 0.88 to 0.9921875
- decay_spike: float32 [4, 128, 32], P('pp', None, 'tp'), may hold values from -2.1 to 0
- per_group_scale: float32 [4, 64], P('pp'), may hold values from 0.1 to 1.9
Outputs:
- outputs: bfloat16 [256, 2048], P('pp', 'tp')
The draws below stay inside these ranges and needn't reach their ends.
All inputs are finite; a program needn't handle non-finite values.
Results may differ from the reference program's by a relative error of at most 0.03.
Values may be sent and summed in bfloat16 or wider, within the bound.
A program may use at most 64 MiB of HBM per device.

```python
import math
import jax
import jax.numpy as jnp
from jax import lax

HEADS = 32
HEAD = 64
D = 2048
SEG = 64
MB_TOK = 128
SECTIONS = 4
MICRO = 2


def draw_entry_stream_rows(key, part):
    first_key, second_key, third_key = jax.random.split(jax.random.fold_in(key, 11), 3)
    rows = MICRO * MB_TOK
    column = jnp.arange(D, dtype=jnp.float32) / D
    values = jnp.clip(jax.random.normal(first_key, (rows, D), jnp.float32), -4.0, 4.0)
    row_scale = jnp.exp(jax.random.uniform(second_key, (rows, 1), jnp.float32, math.log(0.5), math.log(2.0)))
    rising = 3.0 ** (column - 0.5)
    col_scale = rising[None, :] * jnp.exp(jax.random.uniform(third_key, (1, D), jnp.float32, -0.35, 0.35))
    return (values * row_scale * col_scale).astype(jnp.bfloat16)


def draw_retention_minimum(key, part):
    first_key, second_key, third_key = jax.random.split(jax.random.fold_in(key, 23), 3)
    slow_share = 0.5
    slow_heads = jax.random.uniform(first_key, (SECTIONS, HEADS, 1), jnp.float32) < slow_share
    slow_gap = jnp.exp(jax.random.uniform(second_key, (SECTIONS, HEADS, HEAD), jnp.float32, math.log(1.0 / MB_TOK), math.log(4.0 / MB_TOK)))
    fast_gap = jnp.exp(jax.random.uniform(third_key, (SECTIONS, HEADS, HEAD), jnp.float32, math.log(0.04), math.log(0.12)))
    gap_all = jnp.where(slow_heads, slow_gap, fast_gap)
    return (1.0 - gap_all).reshape(SECTIONS, D).astype(jnp.float32)


def draw_decay_spike(key, part):
    first_key, second_key = jax.random.split(jax.random.fold_in(key, 37), 2)
    where_at = jax.random.randint(first_key, (SECTIONS, 3, HEADS), 0, MB_TOK)
    strength = jnp.log(jax.random.uniform(second_key, (SECTIONS, 3, HEADS), jnp.float32, 0.5, 0.8))
    positions = jnp.arange(MB_TOK, dtype=jnp.int32)[None, :, None, None]
    hit_mask = where_at[:, None, :, :] == positions
    return jnp.sum(jnp.where(hit_mask, strength[:, None, :, :], 0.0), axis=2).astype(jnp.float32)


def steps_of(own_key, shape, cuts, least, top_value):
    gain, own = 1.0, jax.random.fold_in(own_key, 6)
    for dim, blocks in cuts:
        heights = jnp.exp(jax.random.uniform(jax.random.fold_in(own, dim), (blocks,), jnp.float32, least / len(cuts), top_value / len(cuts)))
        gain = gain * jnp.repeat(heights, shape[dim] // blocks).reshape([-1 if axis == dim else 1 for axis in range(len(shape))])
    return gain


def normal_values(key, extent, spread, bound, cuts=(), kind=jnp.bfloat16):
    array = jax.random.normal(key, extent, jnp.float32) * spread
    if len(cuts) > 0:
        array = steps_of(key, extent, cuts, -0.22, 0.18) * array
    return jnp.clip(array, min=-bound, max=bound).astype(kind)


def setup_inputs(seed: int = 0) -> dict:
    keys = jax.random.split(jax.random.key(seed), 10)
    entry_stream_rows = draw_entry_stream_rows(jax.random.fold_in(keys[9], 71), 0)
    layer_rescale_factor = jnp.clip(1.0 + 0.18 * jax.random.normal(keys[1], (SECTIONS, D), jnp.float32), 0.1, 1.9)
    probe_projection = normal_values(keys[2], (SECTIONS, D, D), D ** -0.5, 0.125, ((0, 4), (1, 8)))
    retention_projection = normal_values(keys[3], (SECTIONS, D, D), D ** -0.5, 0.125, ((0, 4), (1, 8)))
    candidate_projection = normal_values(keys[4], (SECTIONS, D, D), D ** -0.5, 0.125, ((0, 4), (1, 8)))
    emission_filter_matrix = normal_values(keys[5], (SECTIONS, D, D), D ** -0.5, 0.125, ((0, 4), (1, 8)))
    retention_minimum = draw_retention_minimum(jax.random.fold_in(keys[9], 71), 0)
    decay_spike = draw_decay_spike(jax.random.fold_in(keys[9], 71), 0)
    per_group_scale = jnp.clip(1.0 + 0.18 * jax.random.normal(keys[8], (SECTIONS, HEAD), jnp.float32), 0.1, 1.9)
    return dict(entry_stream_rows=entry_stream_rows, layer_rescale_factor=layer_rescale_factor, probe_projection=probe_projection, retention_projection=retention_projection, candidate_projection=candidate_projection, emission_filter_matrix=emission_filter_matrix, retention_minimum=retention_minimum, decay_spike=decay_spike, per_group_scale=per_group_scale)


EPSILON = 1e-06
HIGHEST = lax.Precision.HIGHEST

def segment_scan(queries, key_in, log_forget, values, memory):
    head_count = queries.shape[0]
    length = queries.shape[1]
    blocks_count = length // SEG

    def split_blocks(tensor):
        return tensor.reshape(head_count, blocks_count, SEG, tensor.shape[-1]).transpose(1, 0, 2, 3)
    lower_mask = jnp.tril(jnp.ones((SEG, SEG), dtype=bool))[None]

    def one_block(memory_in, pieces):
        block_query, block_key, block_forget, block_value = pieces
        running = jnp.cumsum(block_forget, axis=1)
        query_scaled = block_query * jnp.exp(running)
        key_scaled = block_key * jnp.exp(-running)
        scores = jnp.einsum('hid,hjd->hij', query_scaled, key_scaled, precision=HIGHEST)
        scores = jnp.where(lower_mask, scores, 0.0)
        mixed_out = jnp.einsum('hij,hjv->hiv', scores, block_value, precision=HIGHEST)
        mixed_out = mixed_out + jnp.einsum('hid,hdv->hiv', query_scaled, memory_in, precision=HIGHEST)
        ending = running[:, -1:, :]
        carried_in = jnp.einsum('hjd,hjv->hdv', block_key * jnp.exp(ending - running), block_value, precision=HIGHEST)
        memory_out = jnp.exp(ending[:, 0, :])[:, :, None] * memory_in + carried_in
        return (memory_out, mixed_out)
    memory, mixed_out = lax.scan(one_block, memory, (split_blocks(queries), split_blocks(key_in), split_blocks(log_forget), split_blocks(values)))
    return (mixed_out.transpose(1, 0, 2, 3).reshape(head_count, length, values.shape[-1]), memory)

def head_norm(mixed_out, channel_gain):
    return mixed_out * lax.rsqrt(lax.optimization_barrier(jnp.mean(mixed_out * mixed_out, axis=-1, keepdims=True)) + EPSILON) * channel_gain

def reference(entry_stream_rows, layer_rescale_factor, probe_projection, retention_projection, candidate_projection, emission_filter_matrix, retention_minimum, decay_spike, per_group_scale):
    stream = entry_stream_rows
    for layer_ordinal in range(SECTIONS):
        wide_stream = stream.astype(jnp.float32)
        scaled = (wide_stream * layer_rescale_factor[layer_ordinal][None, :]).astype(jnp.bfloat16)
        inverse = lax.rsqrt(lax.optimization_barrier(jnp.mean(wide_stream * wide_stream, axis=1, keepdims=True)) + EPSILON)

        def per_head(tensor):
            return tensor.reshape(MICRO, MB_TOK, HEADS, HEAD).transpose(0, 2, 1, 3)
        projected = []
        for matrix in (probe_projection, retention_projection, candidate_projection, emission_filter_matrix):
            product = jnp.dot(scaled, matrix[layer_ordinal].T, preferred_element_type=jnp.float32) * inverse
            projected.append(per_head(product))
        query_pre, forget_pre, input_pre, gate_pre = projected
        lower_edge = retention_minimum[layer_ordinal].reshape(1, HEADS, 1, HEAD)
        remaining_portion = decay_spike[layer_ordinal].T[None, :, :, None]
        log_forget = jnp.logaddexp(jnp.log(lower_edge), jnp.log1p(-lower_edge) + jax.nn.log_sigmoid(forget_pre)) + remaining_portion
        key_in = (1.0 - lower_edge) * jax.nn.sigmoid(-forget_pre)
        queries = jax.nn.silu(query_pre)

        def one_sequence(pieces):
            zero_state = jnp.zeros((HEADS, HEAD, HEAD), jnp.float32)
            mixed_seq, final_state = segment_scan(pieces[0], pieces[1], pieces[2], pieces[3], zero_state)
            return mixed_seq
        mixed_out = lax.map(one_sequence, (queries, key_in, log_forget, input_pre))
        branch = head_norm(mixed_out, per_group_scale[layer_ordinal]) * jax.nn.silu(gate_pre)
        branch = branch.transpose(0, 2, 1, 3).reshape(MICRO * MB_TOK, D)
        stream = (wide_stream + branch).astype(jnp.bfloat16)
    return stream
```

```python
import functools

import jax
import jax.numpy as jnp
from jax import lax
from jax.experimental import pallas as pl
from jax.experimental.pallas import tpu as pltpu
from jax.sharding import PartitionSpec as P

HEAD = 64
TILE = 256
EPSILON = 1e-06
F32 = jnp.float32
BF16 = jnp.bfloat16
NT = (((1,), (1,)), ((), ()))
NN = (((1,), (0,)), ((), ()))
TN = (((0,), (0,)), ((), ()))


def mm(a, b, dims):
    return lax.dot_general(a, b, dims, preferred_element_type=F32)


def sigmoid(v):
    return 1.0 / (1.0 + jnp.exp(-v))


def at(stage, lane):
    return {"pp": stage, "tp": lane}


def kernel(
    stages,
    lanes_axis,
    x_ref,
    gain_ref,
    wq_ref,
    wf_ref,
    wi_ref,
    wg_ref,
    low_ref,
    spike_ref,
    scale_ref,
    out_ref,
    xv,
    gain_v,
    scale_v,
    lows,
    spike_raw,
    weights,
    turned,
    buf,
    res,
    spikes,
    state,
    outv,
    load_sem,
    w_sem,
    swap_send,
    swap_recv,
    in_send,
    direct_sem,
    forward_sem,
    forward_send,
    send_sem,
    out_sem,
):
    rows, cols = xv.shape
    size = buf.shape[4]
    heads = cols // HEAD
    width = gain_v.shape[1]
    positions = spike_raw.shape[2]
    parts = positions // size
    spans = positions // rows
    chips = lanes_axis // 2
    slots = stages
    last = stages - 1
    stage = lax.axis_index("pp")
    lane = lax.axis_index("tp")
    core = lax.rem(lane, 2)
    other = 1 - core
    z = lane // 2
    partner = z * 2 + other

    barrier = pltpu.get_barrier_semaphore()
    for up in range(stages):
        for over in range(lanes_axis):
            if up or over:
                pl.semaphore_signal(
                    barrier,
                    inc=1,
                    device_id=at(
                        lax.rem(stage + up, stages), lax.rem(lane + over, lanes_axis)
                    ),
                    device_id_type=pl.DeviceIdType.MESH,
                )

    small = [
        pltpu.make_async_copy(gain_ref, gain_v, load_sem.at[1]),
        pltpu.make_async_copy(scale_ref, scale_v, load_sem.at[2]),
        pltpu.make_async_copy(low_ref, lows.at[core], load_sem.at[3]),
        pltpu.make_async_copy(spike_ref.at[0], spike_raw.at[core], load_sem.at[4]),
    ]
    x_load = pltpu.make_async_copy(x_ref, xv, load_sem.at[0])
    x_load.start()
    for load in small:
        load.start()
    loads = []
    for role, ref in enumerate((wq_ref, wf_ref, wi_ref, wg_ref)):
        load = pltpu.make_async_copy(
            ref.at[0], weights.at[pl.ds(role * cols, cols)], w_sem.at[role]
        )
        load.start()
        loads.append(load)

    sequence = stage // spans
    in_parity = lax.rem(sequence, 2)
    in_slot = (sequence // 2) * parts + lax.rem(stage, spans) * 2

    def farthest_first(send):
        for far in range(chips - 1, 0, -1):

            @pl.when(z + far < chips)
            def _():
                send(z + far)

            @pl.when(z - far >= 0)
            def _():
                send(z - far)

    def to_first(target, half):
        return pltpu.make_async_remote_copy(
            src_ref=xv.at[pl.ds(half * size, size)],
            dst_ref=buf.at[in_parity, in_slot + half, core, z],
            send_sem=in_send.at[target],
            recv_sem=direct_sem.at[in_parity, in_slot + half],
            device_id=at(0, target * 2 + core),
            device_id_type=pl.DeviceIdType.MESH,
        )

    def enter():
        for half in range(2):
            farthest_first(lambda target: to_first(target, half).start())

            @pl.when(stage != 0)
            def _():
                to_first(z, half).start()

            @pl.when(stage == 0)
            def _():
                pltpu.make_async_copy(
                    x_ref.at[pl.ds(half * size, size)],
                    buf.at[in_parity, in_slot + half, core, z],
                    direct_sem.at[in_parity, in_slot + half],
                ).start()

    def swap_small(which):
        src, dst = (
            (lows.at[core], lows.at[core])
            if which == 0
            else (spike_raw.at[core], spike_raw.at[core])
        )
        return pltpu.make_async_remote_copy(
            src_ref=src,
            dst_ref=dst,
            send_sem=swap_send.at[1 + which],
            recv_sem=swap_recv.at[1 + which],
            device_id=at(stage, partner),
            device_id_type=pl.DeviceIdType.MESH,
        )

    def swap_tile(k):
        tile = turned.at[core, pl.ds(pl.multiple_of(k * TILE, TILE), TILE)]
        return pltpu.make_async_remote_copy(
            src_ref=tile,
            dst_ref=tile,
            send_sem=swap_send.at[0],
            recv_sem=swap_recv.at[0],
            device_id=at(stage, partner),
            device_id_type=pl.DeviceIdType.MESH,
        )

    head_of_lane = lax.broadcasted_iota(jnp.int32, (size, cols), 1) // HEAD
    tri_row = lax.broadcasted_iota(jnp.int32, (size, size), 0)
    tri_col = lax.broadcasted_iota(jnp.int32, (size, size), 1)
    tril_ones = jnp.where(tri_row >= tri_col, 1.0, 0.0).astype(BF16)
    tall_row = lax.rem(lax.broadcasted_iota(jnp.int32, (heads * size, size), 0), size)
    tall_col = lax.broadcasted_iota(jnp.int32, (heads * size, size), 1)
    tall_mask = tall_row >= tall_col
    sq_row = lax.broadcasted_iota(jnp.int32, (cols, cols), 0) // HEAD
    sq_col = lax.broadcasted_iota(jnp.int32, (cols, cols), 1) // HEAD
    same_head = sq_row == sq_col
    mean_ones = jnp.where(same_head, 1.0 / HEAD, 0.0).astype(BF16)

    def spread(half):
        for part in range(parts):
            piece = spike_raw[half, :, part * size : (part + 1) * size].T
            wide = jnp.zeros((size, cols), F32)
            for h in range(heads):
                wide = jnp.where(head_of_lane == h, piece[:, h : h + 1], wide)
            spikes[half, part] = wide

    for load in small:
        load.wait()
    x_load.wait()
    spread(core)

    pl.semaphore_wait(barrier, stages * lanes_axis - 1)

    @pl.when(in_slot == 0)
    def _():
        enter()

    @pl.when(stage != 0)
    def _():
        swap_small(0).start()
        swap_small(1).start()

    for load in loads:
        load.wait()

    def turn(k, carry):
        tile = pl.ds(pl.multiple_of(k * TILE, TILE), TILE)
        for role in range(4):
            turned[core, tile, role * cols : (role + 1) * cols] = weights[
                role * cols : (role + 1) * cols, tile
            ].T

        @pl.when((stage != 0) & (k > 0))
        def _():
            swap_tile(k - 1).start()

        return carry

    lax.fori_loop(0, width // TILE, turn, 0)

    @pl.when(in_slot != 0)
    def _():
        enter()

    def whole_wait(ref, sem):
        pltpu.make_async_copy(ref, ref, sem).wait()

    def gather(parity, slot):
        current = jnp.concatenate(
            [buf[parity, slot, k % 2, k // 2] for k in range(lanes_axis)], axis=1
        ).astype(F32)
        squares = jnp.sum(current * current, axis=1, keepdims=True)
        scaled = (current * gain_v[...]).astype(BF16)
        return scaled, lax.rsqrt(squares / width + EPSILON)

    out_gain = jnp.concatenate([scale_v[...]] * heads, axis=1)

    def mix(product, inverse, half, part, memory, stream):
        projected = product * inverse
        query_pre = projected[:, 0 * cols : 1 * cols]
        forget_pre = projected[:, 1 * cols : 2 * cols]
        values = projected[:, 2 * cols : 3 * cols].astype(BF16)
        gate_pre = projected[:, 3 * cols : 4 * cols]

        key_in = (1.0 - lows[half]) * sigmoid(-forget_pre)
        log_forget = jnp.log(1.0 - key_in) + spikes[half, part]
        high = log_forget.astype(BF16)
        low = (log_forget - high.astype(F32)).astype(BF16)
        running = mm(tril_ones, high, NN) + mm(tril_ones, low, NN)
        ending = running[size - 1 : size, :]
        query_scaled = query_pre * sigmoid(query_pre) * jnp.exp(running)
        key_scaled = (key_in * jnp.exp(-running)).astype(BF16)
        key_end = (key_in * jnp.exp(ending - running)).astype(BF16)
        query_bf = query_scaled.astype(BF16)
        tall_query = jnp.concatenate(
            [jnp.where(head_of_lane == h, query_scaled, 0.0).astype(BF16) for h in range(heads)],
            axis=0,
        )
        scores = jnp.where(tall_mask, mm(tall_query, key_scaled, NT), 0.0).astype(BF16)
        tall_mixed = mm(scores, values, NN)
        mixed = mm(query_bf, memory.astype(BF16), NT)
        inner = tall_mixed[0:size]
        for h in range(1, heads):
            inner = jnp.where(head_of_lane == h, tall_mixed[h * size : (h + 1) * size], inner)
        mixed = mixed + inner
        mean_square = mm((mixed * mixed).astype(BF16), mean_ones, NN)
        branch = mixed * lax.rsqrt(mean_square + EPSILON) * out_gain
        branch = branch * (gate_pre * sigmoid(gate_pre))
        return (stream + branch).astype(BF16), (values, key_end, ending)

    def advance(memory, carried):
        values, key_end, ending = carried
        added = jnp.where(same_head, mm(values, key_end, TN), 0.0)
        return memory * jnp.exp(ending) + added

    def to_next(slot, index, parity, half, target, to_core):
        return pltpu.make_async_remote_copy(
            src_ref=res.at[slot, index],
            dst_ref=buf.at[parity, slot, half, z],
            send_sem=send_sem.at[slot, index],
            recv_sem=direct_sem.at[parity, slot],
            device_id=at(lax.rem(stage + 1, stages), target * 2 + to_core),
            device_id_type=pl.DeviceIdType.MESH,
        )

    def forward(parity, slot):
        half = buf.at[parity, slot, core]
        return pltpu.make_async_remote_copy(
            src_ref=half,
            dst_ref=half,
            send_sem=forward_send.at[parity, slot],
            recv_sem=forward_sem.at[parity, slot],
            device_id=at(stage, partner),
            device_id_type=pl.DeviceIdType.MESH,
        )

    @pl.when(stage == 0)
    def _():
        steps = 2 * slots

        def pass_on(t):
            parity, slot = lax.rem(t, 2), t // 2
            whole_wait(buf.at[parity, slot, core], direct_sem.at[parity, slot])
            forward(parity, slot).start()

        pass_on(0)

        def step(t, carry):
            parity, slot = lax.rem(t, 2), t // 2
            part = lax.rem(slot, parts)
            whole_wait(buf.at[parity, slot, other], forward_sem.at[parity, slot])
            scaled, inverse = gather(parity, slot)
            product = mm(scaled, turned[core], NN)

            @pl.when(t + 1 < steps)
            def _():
                pass_on(t + 1)

            memory = jnp.where(part == 0, 0.0, state[parity])
            stream = buf[parity, slot, core, z].astype(F32)
            result, carried = mix(product, inverse, core, part, memory, stream)
            res[slot, parity] = result
            to_core = 1 - parity
            farthest_first(
                lambda target: to_next(slot, parity, parity, core, target, to_core).start()
            )
            to_next(slot, parity, parity, core, z, to_core).start()
            state[parity] = advance(memory, carried)
            return carry

        lax.fori_loop(0, steps, step, 0)

        def drain(t, carry):
            parity, slot = lax.rem(t, 2), t // 2
            forward(parity, slot).wait_send()
            whole_wait(buf.at[parity, slot, core], send_sem.at[slot, parity])
            return carry

        lax.fori_loop(0, steps, drain, 0)

    @pl.when(stage != 0)
    def _():
        tiles = width // TILE
        swap_tile(tiles - 1).start()
        swap_small(0).wait_recv()
        swap_small(1).wait_recv()
        spread(other)
        whole_wait(turned.at[other], swap_recv.at[0])
        parity = lax.rem(core + stage, 2)

        def to_out(slot, half):
            part = lax.rem(slot, parts)
            where = ((slot // parts) * 2 + parity) * spans + part // 2
            return where, lax.rem(part, 2)

        def out_copy(slot, half):
            where, low_high = to_out(slot, half)
            return pltpu.make_async_remote_copy(
                src_ref=res.at[slot, half],
                dst_ref=outv.at[low_high],
                send_sem=send_sem.at[slot, half],
                recv_sem=out_sem,
                device_id=at(where, z * 2 + half),
                device_id_type=pl.DeviceIdType.MESH,
            )

        def stays(slot, half):
            where, _ = to_out(slot, half)
            return (where == stage) & (core == half)

        def step(slot, carry):
            part = lax.rem(slot, parts)
            whole_wait(buf.at[parity, slot], direct_sem.at[parity, slot])
            scaled, inverse = gather(parity, slot)
            kept = []
            for half in range(2):
                product = mm(scaled, turned[half], NN)
                memory = jnp.where(part == 0, 0.0, state[half])
                stream = buf[parity, slot, half, z].astype(F32)
                result, carried = mix(product, inverse, half, part, memory, stream)
                res[slot, half] = result
                kept.append((memory, carried))

            @pl.when(stage != last)
            def _():
                for half in range(2):
                    farthest_first(
                        lambda target: to_next(
                            slot, half, parity, half, target, other
                        ).start()
                    )
                    to_next(slot, half, parity, half, z, other).start()

            for half in range(2):

                @pl.when((stage == last) & ~stays(slot, half))
                def _():
                    out_copy(slot, half).start()

                @pl.when((stage == last) & stays(slot, half))
                def _():
                    _, low_high = to_out(slot, half)
                    pltpu.make_async_copy(
                        res.at[slot, half], outv.at[low_high], out_sem
                    ).start()

            for half in range(2):
                memory, carried = kept[half]
                state[half] = advance(memory, carried)
            return carry

        lax.fori_loop(0, slots, step, 0)

        def drain(slot, carry):
            for half in range(2):

                @pl.when(stage != last)
                def _():
                    whole_wait(buf.at[0, 0, 0], send_sem.at[slot, half])

                @pl.when((stage == last) & ~stays(slot, half))
                def _():
                    out_copy(slot, half).wait_send()

            return carry

        lax.fori_loop(0, slots, drain, 0)
        whole_wait(turned.at[core], swap_send.at[0])
        swap_small(0).wait_send()
        swap_small(1).wait_send()

    for target in range(chips):

        @pl.when((stage != 0) | (z != target))
        def _():
            whole_wait(xv, in_send.at[target])

    whole_wait(outv, out_sem)
    for half in range(2):
        out_ref[half * size : (half + 1) * size] = outv[half]


def solution(mesh):
    stages = mesh.shape["pp"]
    lanes_axis = mesh.shape["tp"]
    chips = lanes_axis // 2

    def step(x, gain, wq, wf, wi, wg, low, spike, scale):
        rows, cols = x.shape
        width = gain.shape[1]
        positions = spike.shape[1]
        heads = cols // HEAD
        size = rows // 2
        parts = positions // size
        vmem = pl.BlockSpec(memory_space=pltpu.VMEM)
        hbm = pl.BlockSpec(memory_space=pl.ANY)
        dma = pltpu.SemaphoreType.DMA
        return pl.pallas_call(
            functools.partial(kernel, stages, lanes_axis),
            out_shape=jax.ShapeDtypeStruct((rows, cols), BF16),
            in_specs=[hbm] * 9,
            out_specs=vmem,
            scratch_shapes=[
                pltpu.VMEM((rows, cols), BF16),
                pltpu.VMEM((1, width), F32),
                pltpu.VMEM(scale.shape, F32),
                pltpu.VMEM((2, 1, cols), F32),
                pltpu.VMEM((2, heads, positions), F32),
                pltpu.VMEM((4 * cols, width), BF16),
                pltpu.VMEM((2, width, 4 * cols), BF16),
                pltpu.VMEM((2, stages, 2, chips, size, cols), BF16),
                pltpu.VMEM((stages, 2, size, cols), BF16),
                pltpu.VMEM((2, parts, size, cols), F32),
                pltpu.VMEM((2, cols, cols), F32),
                pltpu.VMEM((2, size, cols), BF16),
                dma((5,)),
                dma((4,)),
                dma((3,)),
                dma((3,)),
                dma((chips,)),
                dma((2, stages)),
                dma((2, stages)),
                dma((2, stages)),
                dma((stages, 2)),
                dma,
            ],
            compiler_params=pltpu.CompilerParams(
                collective_id=0, has_side_effects=True, vmem_limit_bytes=67043328
            ),
        )(x, gain, wq, wf, wi, wg, low, spike.transpose(0, 2, 1), scale)

    in_specs = (
        P("pp", "tp"),
        P("pp", None),
        P("pp", "tp", None),
        P("pp", "tp", None),
        P("pp", "tp", None),
        P("pp", "tp", None),
        P("pp", "tp"),
        P("pp", None, "tp"),
        P("pp", None),
    )
    return jax.shard_map(
        step, mesh=mesh, in_specs=in_specs, out_specs=P("pp", "tp"), check_vma=False
    )
```

```python
import functools

import jax
import jax.numpy as jnp
from jax import lax
from jax.experimental import pallas as pl
from jax.experimental.pallas import tpu as pltpu
from jax.sharding import PartitionSpec as P

HEAD = 64
TILE = 256
EPSILON = 1e-06
GRANT = 40 * 2**20
F32 = jnp.float32
BF16 = jnp.bfloat16
NT = (((1,), (1,)), ((), ()))
NN = (((1,), (0,)), ((), ()))
TN = (((0,), (0,)), ((), ()))


def mm(a, b, dims):
    return lax.dot_general(a, b, dims, preferred_element_type=F32)


def sigmoid(v):
    return 1.0 / (1.0 + jnp.exp(-v))


def at(stage, lane):
    return {"pp": stage, "tp": lane}


def kernel(
    stages,
    lanes_axis,
    x_ref,
    gain_ref,
    wq_ref,
    wf_ref,
    wi_ref,
    wg_ref,
    low_ref,
    spike_ref,
    scale_ref,
    out_ref,
    xv,
    gain_v,
    scale_v,
    lows,
    spike_raw,
    weights,
    turned,
    buf,
    res,
    spikes,
    state,
    load_sem,
    w_sem,
    swap_send,
    swap_recv,
    in_send,
    direct_sem,
    forward_sem,
    forward_send,
    send_sem,
    out_sem,
):
    rows, cols = xv.shape
    size = buf.shape[4]
    heads = cols // HEAD
    width = gain_v.shape[1]
    positions = spike_raw.shape[2]
    parts = positions // size
    spans = positions // rows
    chips = lanes_axis // 2
    slots = stages
    last = stages - 1
    stage = lax.axis_index("pp")
    lane = lax.axis_index("tp")
    core = lax.rem(lane, 2)
    other = 1 - core
    z = lane // 2
    partner = z * 2 + other

    barrier = pltpu.get_barrier_semaphore()
    for up in range(stages):
        for over in range(lanes_axis):
            if up or over:
                pl.semaphore_signal(
                    barrier,
                    inc=1,
                    device_id=at(
                        lax.rem(stage + up, stages), lax.rem(lane + over, lanes_axis)
                    ),
                    device_id_type=pl.DeviceIdType.MESH,
                )

    small = [
        pltpu.make_async_copy(gain_ref, gain_v, load_sem.at[1]),
        pltpu.make_async_copy(scale_ref, scale_v, load_sem.at[2]),
        pltpu.make_async_copy(low_ref, lows.at[core], load_sem.at[3]),
        pltpu.make_async_copy(spike_ref.at[0], spike_raw.at[core], load_sem.at[4]),
    ]
    x_load = pltpu.make_async_copy(x_ref, xv, load_sem.at[0])
    x_load.start()
    for load in small:
        load.start()
    loads = []
    for role, ref in enumerate((wq_ref, wf_ref, wi_ref, wg_ref)):
        load = pltpu.make_async_copy(
            ref.at[0], weights.at[pl.ds(role * cols, cols)], w_sem.at[role]
        )
        load.start()
        loads.append(load)

    sequence = stage // spans
    in_parity = lax.rem(sequence, 2)
    in_slot = (sequence // 2) * parts + lax.rem(stage, spans) * 2

    def farthest_first(send):
        for far in range(chips - 1, 0, -1):

            @pl.when(z + far < chips)
            def _():
                send(z + far)

            @pl.when(z - far >= 0)
            def _():
                send(z - far)

    def to_first(target, half):
        return pltpu.make_async_remote_copy(
            src_ref=xv.at[pl.ds(half * size, size)],
            dst_ref=buf.at[in_slot + half, in_parity, core, z],
            send_sem=in_send.at[target],
            recv_sem=direct_sem.at[in_slot + half],
            device_id=at(0, target * 2 + core),
            device_id_type=pl.DeviceIdType.MESH,
        )

    def enter():
        for half in range(2):
            farthest_first(lambda target: to_first(target, half).start())

            @pl.when(stage != 0)
            def _():
                to_first(z, half).start()

            @pl.when(stage == 0)
            def _():
                pltpu.make_async_copy(
                    x_ref.at[pl.ds(half * size, size)],
                    buf.at[in_slot + half, in_parity, core, z],
                    direct_sem.at[in_slot + half],
                ).start()

    def swap_small(which):
        src, dst = (
            (lows.at[core], lows.at[core])
            if which == 0
            else (spike_raw.at[core], spike_raw.at[core])
        )
        return pltpu.make_async_remote_copy(
            src_ref=src,
            dst_ref=dst,
            send_sem=swap_send.at[1 + which],
            recv_sem=swap_recv.at[1 + which],
            device_id=at(stage, partner),
            device_id_type=pl.DeviceIdType.MESH,
        )

    def swap_tile(k):
        tile = turned.at[core, pl.ds(pl.multiple_of(k * TILE, TILE), TILE)]
        return pltpu.make_async_remote_copy(
            src_ref=tile,
            dst_ref=tile,
            send_sem=swap_send.at[0],
            recv_sem=swap_recv.at[0],
            device_id=at(stage, partner),
            device_id_type=pl.DeviceIdType.MESH,
        )

    head_of_lane = lax.broadcasted_iota(jnp.int32, (size, cols), 1) // HEAD
    tri_row = lax.broadcasted_iota(jnp.int32, (size, size), 0)
    tri_col = lax.broadcasted_iota(jnp.int32, (size, size), 1)
    tril_ones = jnp.where(tri_row >= tri_col, 1.0, 0.0).astype(BF16)
    tall_row = lax.rem(lax.broadcasted_iota(jnp.int32, (heads * size, size), 0), size)
    tall_col = lax.broadcasted_iota(jnp.int32, (heads * size, size), 1)
    tall_mask = tall_row >= tall_col
    sq_row = lax.broadcasted_iota(jnp.int32, (cols, cols), 0) // HEAD
    sq_col = lax.broadcasted_iota(jnp.int32, (cols, cols), 1) // HEAD
    same_head = sq_row == sq_col
    mean_ones = jnp.where(same_head, 1.0 / HEAD, 0.0).astype(BF16)

    def spread(half):
        for part in range(parts):
            piece = spike_raw[half, :, part * size : (part + 1) * size].T
            wide = jnp.zeros((size, cols), F32)
            for h in range(heads):
                wide = jnp.where(head_of_lane == h, piece[:, h : h + 1], wide)
            spikes[half, part] = wide

    x_load.wait()
    pl.semaphore_wait(barrier, stages * lanes_axis - 1)

    @pl.when(in_slot == 0)
    def _():
        enter()

    for load in small:
        load.wait()

    @pl.when(stage != 0)
    def _():
        swap_small(0).start()
        swap_small(1).start()

    spread(core)
    for load in loads:
        load.wait()

    def turn(k, carry):
        tile = pl.ds(pl.multiple_of(k * TILE, TILE), TILE)
        for role in range(4):
            turned[core, tile, role * cols : (role + 1) * cols] = weights[
                role * cols : (role + 1) * cols, tile
            ].T

        @pl.when((stage != 0) & (k > 0))
        def _():
            swap_tile(k - 1).start()

        return carry

    lax.fori_loop(0, width // TILE, turn, 0)

    @pl.when(in_slot != 0)
    def _():
        enter()

    def whole_wait(ref, sem):
        pltpu.make_async_copy(ref, ref, sem).wait()

    def gather(slot, parities):
        current = jnp.concatenate(
            [
                jnp.concatenate(
                    [buf[slot, parity, k % 2, k // 2] for k in range(lanes_axis)], axis=1
                )
                for parity in parities
            ],
            axis=0,
        ).astype(F32)
        squares = jnp.sum(current * current, axis=1, keepdims=True)
        scaled = (current * gain_v[...]).astype(BF16)
        return scaled, lax.rsqrt(squares / width + EPSILON)

    out_gain = jnp.concatenate([scale_v[...]] * heads, axis=1)

    def mix(product, inverse, half, part, memory, stream):
        projected = product * inverse
        query_pre = projected[:, 0 * cols : 1 * cols]
        forget_pre = projected[:, 1 * cols : 2 * cols]
        values = projected[:, 2 * cols : 3 * cols].astype(BF16)
        gate_pre = projected[:, 3 * cols : 4 * cols]

        key_in = (1.0 - lows[half]) * sigmoid(-forget_pre)
        log_forget = jnp.log(1.0 - key_in) + spikes[half, part]
        high = log_forget.astype(BF16)
        low = (log_forget - high.astype(F32)).astype(BF16)
        running = mm(tril_ones, high, NN) + mm(tril_ones, low, NN)
        ending = running[size - 1 : size, :]
        query_scaled = query_pre * sigmoid(query_pre) * jnp.exp(running)
        key_scaled = (key_in * jnp.exp(-running)).astype(BF16)
        key_end = (key_in * jnp.exp(ending - running)).astype(BF16)
        query_bf = query_scaled.astype(BF16)
        tall_query = jnp.concatenate(
            [jnp.where(head_of_lane == h, query_scaled, 0.0).astype(BF16) for h in range(heads)],
            axis=0,
        )
        scores = jnp.where(tall_mask, mm(tall_query, key_scaled, NT), 0.0).astype(BF16)
        tall_mixed = mm(scores, values, NN)
        mixed = mm(query_bf, memory.astype(BF16), NT)
        inner = tall_mixed[0:size]
        for h in range(1, heads):
            inner = jnp.where(head_of_lane == h, tall_mixed[h * size : (h + 1) * size], inner)
        mixed = mixed + inner
        mean_square = mm((mixed * mixed).astype(BF16), mean_ones, NN)
        branch = mixed * lax.rsqrt(mean_square + EPSILON) * out_gain
        branch = branch * (gate_pre * sigmoid(gate_pre))
        return (stream + branch).astype(BF16), (values, key_end, ending)

    def advance(memory, carried):
        values, key_end, ending = carried
        added = jnp.where(same_head, mm(values, key_end, TN), 0.0)
        return memory * jnp.exp(ending) + added

    @pl.when(stage == 0)
    def _():
        def to_next(slot, parity, target):
            return pltpu.make_async_remote_copy(
                src_ref=res.at[slot, parity],
                dst_ref=buf.at[slot, parity, core, z],
                send_sem=send_sem.at[slot],
                recv_sem=direct_sem.at[slot],
                device_id=at(1, target * 2 + 1 - parity),
                device_id_type=pl.DeviceIdType.MESH,
            )

        def forward(slot):
            half = buf.at[slot, :, core]
            return pltpu.make_async_remote_copy(
                src_ref=half,
                dst_ref=half,
                send_sem=forward_send.at[slot],
                recv_sem=forward_sem.at[slot],
                device_id=at(stage, partner),
                device_id_type=pl.DeviceIdType.MESH,
            )

        def pass_on(slot):
            whole_wait(buf.at[slot, :, core], direct_sem.at[slot])
            forward(slot).start()

        pass_on(0)

        def step(slot, carry):
            part = lax.rem(slot, parts)
            whole_wait(buf.at[slot, :, other], forward_sem.at[slot])
            scaled, inverse = gather(slot, (0, 1))
            product = mm(scaled, turned[core], NN)

            @pl.when(slot + 1 < slots)
            def _():
                pass_on(slot + 1)

            for parity in range(2):
                own = slice(parity * size, (parity + 1) * size)
                memory = jnp.where(part == 0, 0.0, state[parity])
                stream = buf[slot, parity, core, z].astype(F32)
                result, carried = mix(product[own], inverse[own], core, part, memory, stream)
                res[slot, parity] = result
                farthest_first(lambda target: to_next(slot, parity, target).start())
                to_next(slot, parity, z).start()
                state[parity] = advance(memory, carried)
            return carry

        lax.fori_loop(0, slots, step, 0)

        def drain(slot, carry):
            forward(slot).wait_send()
            whole_wait(buf.at[slot, 0], send_sem.at[slot])
            return carry

        lax.fori_loop(0, slots, drain, 0)

    @pl.when(stage != 0)
    def _():
        tiles = width // TILE
        swap_tile(tiles - 1).start()
        swap_small(0).wait_recv()
        swap_small(1).wait_recv()
        spread(other)
        whole_wait(turned.at[other], swap_recv.at[0])
        parity = lax.rem(core + stage, 2)

        def to_next(slot, target):
            return pltpu.make_async_remote_copy(
                src_ref=res.at[slot],
                dst_ref=buf.at[slot, parity, :, z],
                send_sem=send_sem.at[slot],
                recv_sem=direct_sem.at[slot],
                device_id=at(lax.rem(stage + 1, stages), target * 2 + other),
                device_id_type=pl.DeviceIdType.MESH,
            )

        def owner(slot):
            part = lax.rem(slot, parts)
            return ((slot // parts) * 2 + parity) * spans + part // 2

        def place(slot):
            start = pl.multiple_of(lax.rem(slot, 2) * size, size)
            return out_ref.at[pl.ds(start, size)]

        def out_copy(slot, half):
            return pltpu.make_async_remote_copy(
                src_ref=res.at[slot, half],
                dst_ref=place(slot),
                send_sem=send_sem.at[slot],
                recv_sem=out_sem,
                device_id=at(owner(slot), z * 2 + half),
                device_id_type=pl.DeviceIdType.MESH,
            )

        def stays(slot, half):
            return (owner(slot) == stage) & (core == half)

        def step(slot, carry):
            part = lax.rem(slot, parts)
            whole_wait(buf.at[slot, parity], direct_sem.at[slot])
            scaled, inverse = gather(slot, (parity,))
            kept = []
            for half in range(2):
                product = mm(scaled, turned[half], NN)
                memory = jnp.where(part == 0, 0.0, state[half])
                stream = buf[slot, parity, half, z].astype(F32)
                result, carried = mix(product, inverse, half, part, memory, stream)
                res[slot, half] = result
                kept.append((memory, carried))

            @pl.when(stage != last)
            def _():
                farthest_first(lambda target: to_next(slot, target).start())
                to_next(slot, z).start()

            for half in range(2):

                @pl.when((stage == last) & ~stays(slot, half))
                def _():
                    out_copy(slot, half).start()

                @pl.when((stage == last) & stays(slot, half))
                def _():
                    pltpu.make_async_copy(res.at[slot, half], place(slot), out_sem).start()

            for half in range(2):
                memory, carried = kept[half]
                state[half] = advance(memory, carried)
            return carry

        lax.fori_loop(0, slots, step, 0)

        def drain(slot, carry):
            @pl.when(stage != last)
            def _():
                whole_wait(buf.at[slot, 0], send_sem.at[slot])

            for half in range(2):

                @pl.when((stage == last) & ~stays(slot, half))
                def _():
                    out_copy(slot, half).wait_send()

            return carry

        lax.fori_loop(0, slots, drain, 0)
        whole_wait(turned.at[core], swap_send.at[0])
        swap_small(0).wait_send()
        swap_small(1).wait_send()

    for target in range(chips):

        @pl.when((stage != 0) | (z != target))
        def _():
            whole_wait(xv, in_send.at[target])

    whole_wait(out_ref, out_sem)


def solution(mesh):
    stages = mesh.shape["pp"]
    lanes_axis = mesh.shape["tp"]
    chips = lanes_axis // 2

    def step(x, gain, wq, wf, wi, wg, low, spike, scale):
        rows, cols = x.shape
        width = gain.shape[1]
        positions = spike.shape[1]
        heads = cols // HEAD
        size = rows // 2
        parts = positions // size
        vmem = pl.BlockSpec(memory_space=pltpu.VMEM)
        hbm = pl.BlockSpec(memory_space=pl.ANY)
        dma = pltpu.SemaphoreType.DMA
        return pl.pallas_call(
            functools.partial(kernel, stages, lanes_axis),
            out_shape=jax.ShapeDtypeStruct((rows, cols), BF16),
            in_specs=[hbm] * 9,
            out_specs=vmem,
            scratch_shapes=[
                pltpu.VMEM((rows, cols), BF16),
                pltpu.VMEM((1, width), F32),
                pltpu.VMEM(scale.shape, F32),
                pltpu.VMEM((2, 1, cols), F32),
                pltpu.VMEM((2, heads, positions), F32),
                pltpu.VMEM((4 * cols, width), BF16),
                pltpu.VMEM((2, width, 4 * cols), BF16),
                pltpu.VMEM((stages, 2, 2, chips, size, cols), BF16),
                pltpu.VMEM((stages, 2, size, cols), BF16),
                pltpu.VMEM((2, parts, size, cols), F32),
                pltpu.VMEM((2, cols, cols), F32),
                dma((5,)),
                dma((4,)),
                dma((3,)),
                dma((3,)),
                dma((chips,)),
                dma((stages,)),
                dma((stages,)),
                dma((stages,)),
                dma((stages,)),
                dma,
            ],
            compiler_params=pltpu.CompilerParams(
                collective_id=0, has_side_effects=True, vmem_limit_bytes=GRANT
            ),
        )(
            *[
                pltpu.with_memory_space_constraint(v, pltpu.HBM)
                for v in (x, gain, wq, wf, wi, wg, low, spike.transpose(0, 2, 1), scale)
            ]
        )

    in_specs = (
        P("pp", "tp"),
        P("pp", None),
        P("pp", "tp", None),
        P("pp", "tp", None),
        P("pp", "tp", None),
        P("pp", "tp", None),
        P("pp", "tp"),
        P("pp", None, "tp"),
        P("pp", None),
    )
    return jax.shard_map(
        step, mesh=mesh, in_specs=in_specs, out_specs=P("pp", "tp"), check_vma=False
    )
```

```python
import functools

import jax
import jax.numpy as jnp
from jax import lax
from jax.experimental import pallas as pl
from jax.experimental.pallas import tpu as pltpu
from jax.sharding import PartitionSpec as P

HEAD = 64
TILE = 256
EPSILON = 1e-06
GRANT = 40 * 2**20
F32 = jnp.float32
BF16 = jnp.bfloat16
NT = (((1,), (1,)), ((), ()))
NN = (((1,), (0,)), ((), ()))
TN = (((0,), (0,)), ((), ()))


def mm(a, b, dims):
    return lax.dot_general(a, b, dims, preferred_element_type=F32)


def sigmoid(v):
    return 1.0 / (1.0 + jnp.exp(-v))


def at(stage, lane):
    return {"pp": stage, "tp": lane}


def kernel(
    stages,
    lanes_axis,
    x_ref,
    gain_ref,
    wq_ref,
    wf_ref,
    wi_ref,
    wg_ref,
    low_ref,
    spike_ref,
    scale_ref,
    out_ref,
    xv,
    gain_v,
    scale_v,
    lows,
    spike_raw,
    weights,
    turned,
    buf,
    res,
    spikes,
    state,
    load_sem,
    w_sem,
    swap_send,
    swap_recv,
    in_send,
    direct_sem,
    forward_sem,
    forward_send,
    send_sem,
    out_sem,
):
    rows, cols = xv.shape
    size = buf.shape[4]
    heads = cols // HEAD
    width = turned.shape[1]
    positions = spike_raw.shape[2]
    parts = positions // size
    spans = positions // rows
    chips = lanes_axis // 2
    slots = stages
    last = stages - 1
    stage = lax.axis_index("pp")
    lane = lax.axis_index("tp")
    core = lax.rem(lane, 2)
    other = 1 - core
    z = lane // 2
    partner = z * 2 + other

    barrier = pltpu.get_barrier_semaphore()

    def ready(to_stage, to_lane):
        pl.semaphore_signal(
            barrier,
            inc=1,
            device_id=at(to_stage, to_lane),
            device_id_type=pl.DeviceIdType.MESH,
        )

    ready(stage, partner)

    @pl.when(stage == 0)
    def _():
        for source in range(stages):
            for over in range(chips):
                ready(source, over * 2 + other)

    @pl.when(stage == 1)
    def _():
        for over in range(lanes_axis):
            ready(0, over)

    @pl.when(stage > 1)
    def _():
        for over in range(chips):
            ready(stage - 1, over * 2 + other)

    ready_from_last = [(last, z * 2 + c) for c in range(2)]
    for c in range(2):

        @pl.when((stage != last) | (core != c))
        def _():
            ready(*ready_from_last[c])

    onward = jnp.where(
        stage == 0,
        2 * chips,
        jnp.where(stage == last, 2 * stages - 1, chips),
    )
    greetings = 1 + chips + onward

    small = [
        pltpu.make_async_copy(scale_ref, scale_v, load_sem.at[2]),
        pltpu.make_async_copy(low_ref, lows.at[core], load_sem.at[3]),
        pltpu.make_async_copy(spike_ref.at[0], spike_raw.at[core], load_sem.at[4]),
    ]
    x_load = pltpu.make_async_copy(x_ref, xv, load_sem.at[0])
    x_load.start()
    for k in range(chips):
        small.append(
            pltpu.make_async_copy(
                gain_ref.at[:, k * 2 * cols : (k + 1) * 2 * cols],
                gain_v.at[k],
                load_sem.at[5 + k],
            )
        )
    for load in small:
        load.start()
    loads = []
    for role, ref in enumerate((wq_ref, wf_ref, wi_ref, wg_ref)):
        load = pltpu.make_async_copy(
            ref.at[0], weights.at[pl.ds(role * cols, cols)], w_sem.at[role]
        )
        load.start()
        loads.append(load)

    sequence = stage // spans
    in_parity = lax.rem(sequence, 2)
    in_slot = (sequence // 2) * parts + lax.rem(stage, spans) * 2

    def farthest_first(send):
        for far in range(chips - 1, 0, -1):

            @pl.when(z + far < chips)
            def _():
                send(z + far)

            @pl.when(z - far >= 0)
            def _():
                send(z - far)

    def to_first(target, half):
        return pltpu.make_async_remote_copy(
            src_ref=xv.at[pl.ds(half * size, size)],
            dst_ref=buf.at[in_slot + half, in_parity, core, z],
            send_sem=in_send.at[target],
            recv_sem=direct_sem.at[in_slot + half, in_parity, z],
            device_id=at(0, target * 2 + other),
            device_id_type=pl.DeviceIdType.MESH,
        )

    def enter(half):
        farthest_first(lambda target: to_first(target, half).start())
        to_first(z, half).start()

    def swap_small(which):
        src, dst = (
            (lows.at[core], lows.at[core])
            if which == 0
            else (spike_raw.at[core], spike_raw.at[core])
        )
        return pltpu.make_async_remote_copy(
            src_ref=src,
            dst_ref=dst,
            send_sem=swap_send.at[1 + which],
            recv_sem=swap_recv.at[1 + which],
            device_id=at(stage, partner),
            device_id_type=pl.DeviceIdType.MESH,
        )

    def swap_tile(k):
        tile = turned.at[core, pl.ds(pl.multiple_of(k * TILE, TILE), TILE)]
        return pltpu.make_async_remote_copy(
            src_ref=tile,
            dst_ref=tile,
            send_sem=swap_send.at[0],
            recv_sem=swap_recv.at[0],
            device_id=at(stage, partner),
            device_id_type=pl.DeviceIdType.MESH,
        )

    head_of_lane = lax.broadcasted_iota(jnp.int32, (size, cols), 1) // HEAD
    tri_row = lax.broadcasted_iota(jnp.int32, (size, size), 0)
    tri_col = lax.broadcasted_iota(jnp.int32, (size, size), 1)
    tril_ones = jnp.where(tri_row >= tri_col, 1.0, 0.0).astype(BF16)
    tall_row = lax.rem(lax.broadcasted_iota(jnp.int32, (heads * size, size), 0), size)
    tall_col = lax.broadcasted_iota(jnp.int32, (heads * size, size), 1)
    tall_mask = tall_row >= tall_col
    sq_row = lax.broadcasted_iota(jnp.int32, (cols, cols), 0) // HEAD
    sq_col = lax.broadcasted_iota(jnp.int32, (cols, cols), 1) // HEAD
    same_head = sq_row == sq_col
    mean_ones = jnp.where(same_head, 1.0 / HEAD, 0.0).astype(BF16)

    def spread(half):
        for part in range(parts):
            piece = spike_raw[half, :, part * size : (part + 1) * size].T
            wide = jnp.zeros((size, cols), F32)
            for h in range(heads):
                wide = jnp.where(head_of_lane == h, piece[:, h : h + 1], wide)
            spikes[half, part] = wide

    x_load.wait()
    pl.semaphore_wait(barrier, greetings)

    @pl.when(in_slot == 0)
    def _():
        enter(0)

    for load in small:
        load.wait()

    @pl.when(stage != 0)
    def _():
        swap_small(0).start()
        swap_small(1).start()

    spread(core)

    @pl.when(in_slot == 0)
    def _():
        enter(1)

    for load in loads:
        load.wait()

    def turn(k, carry):
        tile = pl.ds(pl.multiple_of(k * TILE, TILE), TILE)
        for role in range(4):
            turned[core, tile, role * cols : (role + 1) * cols] = weights[
                role * cols : (role + 1) * cols, tile
            ].T

        @pl.when((stage != 0) & (k > 0))
        def _():
            swap_tile(k - 1).start()

        return carry

    lax.fori_loop(0, width // TILE, turn, 0)

    @pl.when(in_slot != 0)
    def _():
        enter(0)
        enter(1)

    def whole_wait(ref, sem):
        pltpu.make_async_copy(ref, ref, sem).wait()

    def block(slot, parity, k):
        current = jnp.concatenate(
            [buf[slot, parity, c, k] for c in range(2)], axis=1
        ).astype(F32)
        squares = jnp.sum(current * current, axis=1, keepdims=True)
        return (current * gain_v[k]).astype(BF16), squares

    def gather(slot, parity):
        blocks = [block(slot, parity, k) for k in range(chips)]
        scaled = jnp.concatenate([b[0] for b in blocks], axis=1)
        return scaled, inverse_of(sum(b[1] for b in blocks))

    def inverse_of(squares):
        return lax.rsqrt(squares / width + EPSILON)

    out_gain = jnp.concatenate([scale_v[...]] * heads, axis=1)

    def mix(product, inverse, half, part, memory, stream):
        projected = product * inverse
        query_pre = projected[:, 0 * cols : 1 * cols]
        forget_pre = projected[:, 1 * cols : 2 * cols]
        values = projected[:, 2 * cols : 3 * cols].astype(BF16)
        gate_pre = projected[:, 3 * cols : 4 * cols]

        key_in = (1.0 - lows[half]) * sigmoid(-forget_pre)
        log_forget = jnp.log(1.0 - key_in) + spikes[half, part]
        high = log_forget.astype(BF16)
        low = (log_forget - high.astype(F32)).astype(BF16)
        running = mm(tril_ones, high, NN) + mm(tril_ones, low, NN)
        ending = running[size - 1 : size, :]
        query_scaled = query_pre * sigmoid(query_pre) * jnp.exp(running)
        key_scaled = (key_in * jnp.exp(-running)).astype(BF16)
        key_end = (key_in * jnp.exp(ending - running)).astype(BF16)
        query_bf = query_scaled.astype(BF16)
        tall_query = jnp.concatenate(
            [jnp.where(head_of_lane == h, query_scaled, 0.0).astype(BF16) for h in range(heads)],
            axis=0,
        )
        scores = jnp.where(tall_mask, mm(tall_query, key_scaled, NT), 0.0).astype(BF16)
        tall_mixed = mm(scores, values, NN)
        mixed = tall_mixed[0:size]
        for h in range(1, heads):
            mixed = jnp.where(head_of_lane == h, tall_mixed[h * size : (h + 1) * size], mixed)
        if memory is not None:
            mixed = mixed + mm(query_bf, memory.astype(BF16), NT)
        mean_square = mm((mixed * mixed).astype(BF16), mean_ones, NN)
        branch = mixed * lax.rsqrt(mean_square + EPSILON) * out_gain
        branch = branch * (gate_pre * sigmoid(gate_pre))
        return (stream + branch).astype(BF16), (values, key_end, ending)

    def advance(memory, carried):
        values, key_end, ending = carried
        added = jnp.where(same_head, mm(values, key_end, TN), 0.0)
        return added if memory is None else memory * jnp.exp(ending) + added

    @pl.when(stage == 0)
    def _():
        def to_next(slot, parity, target):
            return pltpu.make_async_remote_copy(
                src_ref=res.at[slot, parity],
                dst_ref=buf.at[slot, parity, core, z],
                send_sem=send_sem.at[slot],
                recv_sem=direct_sem.at[slot, parity, z],
                device_id=at(1, target * 2 + 1 - parity),
                device_id_type=pl.DeviceIdType.MESH,
            )

        def forward(slot, parity):
            half = buf.at[slot, parity, other]
            return pltpu.make_async_remote_copy(
                src_ref=half,
                dst_ref=half,
                send_sem=forward_send.at[slot, parity],
                recv_sem=forward_sem.at[slot, parity],
                device_id=at(stage, partner),
                device_id_type=pl.DeviceIdType.MESH,
            )

        def pass_on(slot, parity):
            for k in range(chips):
                whole_wait(buf.at[slot, parity, other, k], direct_sem.at[slot, parity, k])
            forward(slot, parity).start()

        def finish(slot, parity, part, product, inverse, memory):
            stream = buf[slot, parity, core, z].astype(F32)
            result, carried = mix(product, inverse, core, part, memory, stream)
            res[slot, parity] = result
            farthest_first(lambda target: to_next(slot, parity, target).start())
            to_next(slot, parity, z).start()
            state[parity] = advance(memory, carried)

        pass_on(0, 0)

        def single(parity, carry):
            whole_wait(buf.at[0, parity, core], forward_sem.at[0, parity])
            scaled, inverse = gather(0, parity)
            product = mm(scaled, turned[core], NN)

            @pl.when(parity == 0)
            def _():
                pass_on(0, 1)

            @pl.when(parity == 1)
            def _():
                pass_on(1, 0)
                pass_on(1, 1)

            finish(0, parity, 0, product, inverse, None)
            return carry

        lax.fori_loop(0, 2, single, 0)

        def step(slot, carry):
            part = lax.rem(slot, parts)
            for parity in range(2):
                whole_wait(buf.at[slot, parity, core], forward_sem.at[slot, parity])
            both = [gather(slot, parity) for parity in range(2)]
            product = mm(jnp.concatenate([b[0] for b in both], axis=0), turned[core], NN)

            @pl.when(slot + 1 < slots)
            def _():
                pass_on(slot + 1, 0)
                pass_on(slot + 1, 1)

            for parity in range(2):
                memory = jnp.where(part == 0, 0.0, state[parity])
                own = product[parity * size : (parity + 1) * size]
                finish(slot, parity, part, own, both[parity][1], memory)
            return carry

        lax.fori_loop(1, slots, step, 0)

        def drain(slot, carry):
            for parity in range(2):
                forward(slot, parity).wait_send()
            whole_wait(buf.at[slot, 0], send_sem.at[slot])
            return carry

        lax.fori_loop(0, slots, drain, 0)

    @pl.when(stage != 0)
    def _():
        tiles = width // TILE
        swap_tile(tiles - 1).start()
        swap_small(0).wait_recv()
        swap_small(1).wait_recv()
        spread(other)
        whole_wait(turned.at[other], swap_recv.at[0])
        parity = lax.rem(core + stage, 2)
        upper = z // ((chips + 1) // 2)

        def to_next(slot, target):
            return pltpu.make_async_remote_copy(
                src_ref=res.at[slot],
                dst_ref=buf.at[slot, parity, :, z],
                send_sem=send_sem.at[slot],
                recv_sem=direct_sem.at[slot, parity, z],
                device_id=at(lax.rem(stage + 1, stages), target * 2 + other),
                device_id_type=pl.DeviceIdType.MESH,
            )

        def owner(slot):
            part = lax.rem(slot, parts)
            return ((slot // parts) * 2 + parity) * spans + part // 2

        def place(slot):
            start = pl.multiple_of(lax.rem(slot, 2) * size, size)
            return out_ref.at[pl.ds(start, size)]

        def out_copy(slot, half):
            return pltpu.make_async_remote_copy(
                src_ref=res.at[slot, half],
                dst_ref=place(slot),
                send_sem=send_sem.at[slot],
                recv_sem=out_sem,
                device_id=at(owner(slot), z * 2 + half),
                device_id_type=pl.DeviceIdType.MESH,
            )

        def stays(slot, half):
            return (owner(slot) == stage) & (core == half)

        def step(slot, carry):
            part = lax.rem(slot, parts)
            squares, products = 0.0, [0.0, 0.0]
            for j in range(chips):
                k = upper * j + (1 - upper) * (chips - 1 - j)
                whole_wait(buf.at[slot, parity, :, k], direct_sem.at[slot, parity, k])
                scaled, added = block(slot, parity, k)
                squares = squares + added
                span = pl.ds(pl.multiple_of(k * 2 * cols, 2 * cols), 2 * cols)
                for half in range(2):
                    products[half] = products[half] + mm(scaled, turned[half, span], NN)
            inverse = inverse_of(squares)
            kept = []
            for half in range(2):
                product = products[half]
                memory = jnp.where(part == 0, 0.0, state[half])
                stream = buf[slot, parity, half, z].astype(F32)
                result, carried = mix(product, inverse, half, part, memory, stream)
                res[slot, half] = result
                kept.append((memory, carried))

            @pl.when(stage != last)
            def _():
                farthest_first(lambda target: to_next(slot, target).start())
                to_next(slot, z).start()

            for half in range(2):

                @pl.when((stage == last) & ~stays(slot, half))
                def _():
                    out_copy(slot, half).start()

                @pl.when((stage == last) & stays(slot, half))
                def _():
                    pltpu.make_async_copy(res.at[slot, half], place(slot), out_sem).start()

            for half in range(2):
                memory, carried = kept[half]
                state[half] = advance(memory, carried)
            return carry

        lax.fori_loop(0, slots, step, 0)

        def drain(slot, carry):
            @pl.when(stage != last)
            def _():
                whole_wait(buf.at[slot, 0], send_sem.at[slot])

            for half in range(2):

                @pl.when((stage == last) & ~stays(slot, half))
                def _():
                    out_copy(slot, half).wait_send()

            return carry

        lax.fori_loop(0, slots, drain, 0)
        whole_wait(turned.at[core], swap_send.at[0])
        swap_small(0).wait_send()
        swap_small(1).wait_send()

    for target in range(chips):
        whole_wait(xv, in_send.at[target])

    whole_wait(out_ref, out_sem)


def solution(mesh):
    stages = mesh.shape["pp"]
    lanes_axis = mesh.shape["tp"]
    chips = lanes_axis // 2

    def step(x, gain, wq, wf, wi, wg, low, spike, scale):
        rows, cols = x.shape
        width = gain.shape[1]
        positions = spike.shape[1]
        heads = cols // HEAD
        size = rows // 2
        parts = positions // size
        vmem = pl.BlockSpec(memory_space=pltpu.VMEM)
        hbm = pl.BlockSpec(memory_space=pl.ANY)
        dma = pltpu.SemaphoreType.DMA
        return pl.pallas_call(
            functools.partial(kernel, stages, lanes_axis),
            out_shape=jax.ShapeDtypeStruct((rows, cols), BF16),
            in_specs=[hbm] * 9,
            out_specs=vmem,
            scratch_shapes=[
                pltpu.VMEM((rows, cols), BF16),
                pltpu.VMEM((chips, 1, 2 * cols), F32),
                pltpu.VMEM(scale.shape, F32),
                pltpu.VMEM((2, 1, cols), F32),
                pltpu.VMEM((2, heads, positions), F32),
                pltpu.VMEM((4 * cols, width), BF16),
                pltpu.VMEM((2, width, 4 * cols), BF16),
                pltpu.VMEM((stages, 2, 2, chips, size, cols), BF16),
                pltpu.VMEM((stages, 2, size, cols), BF16),
                pltpu.VMEM((2, parts, size, cols), F32),
                pltpu.VMEM((2, cols, cols), F32),
                dma((5 + chips,)),
                dma((4,)),
                dma((3,)),
                dma((3,)),
                dma((chips,)),
                dma((stages, 2, chips)),
                dma((stages, 2)),
                dma((stages, 2)),
                dma((stages,)),
                dma,
            ],
            compiler_params=pltpu.CompilerParams(
                collective_id=0, has_side_effects=True, vmem_limit_bytes=GRANT
            ),
        )(
            *[
                pltpu.with_memory_space_constraint(v, pltpu.HBM)
                for v in (x, gain, wq, wf, wi, wg, low, spike.transpose(0, 2, 1), scale)
            ]
        )

    in_specs = (
        P("pp", "tp"),
        P("pp", None),
        P("pp", "tp", None),
        P("pp", "tp", None),
        P("pp", "tp", None),
        P("pp", "tp", None),
        P("pp", "tp"),
        P("pp", None, "tp"),
        P("pp", None),
    )
    return jax.shard_map(
        step, mesh=mesh, in_specs=in_specs, out_specs=P("pp", "tp"), check_vma=False
    )
```

```python
import functools

import jax
import jax.numpy as jnp
from jax import lax
from jax.experimental import pallas as pl
from jax.experimental.pallas import tpu as pltpu
from jax.sharding import PartitionSpec as P

HEAD = 64
TILE = 256
EPSILON = 1e-06
GRANT = 40 * 2**20
SENT_AFTER = (1, 4)
F32 = jnp.float32
BF16 = jnp.bfloat16
NT = (((1,), (1,)), ((), ()))
NN = (((1,), (0,)), ((), ()))
TN = (((0,), (0,)), ((), ()))


def mm(a, b, dims):
    return lax.dot_general(a, b, dims, preferred_element_type=F32)


def sigmoid(v):
    return 1.0 / (1.0 + jnp.exp(-v))


def at(stage, lane):
    return {"pp": stage, "tp": lane}


def kernel(
    stages,
    lanes_axis,
    x_ref,
    gain_ref,
    wq_ref,
    wf_ref,
    wi_ref,
    wg_ref,
    low_ref,
    spike_ref,
    scale_ref,
    out_ref,
    xv,
    gain_v,
    scale_v,
    lows,
    spike_raw,
    weights,
    turned,
    buf,
    res,
    spikes,
    state,
    load_sem,
    w_sem,
    swap_send,
    swap_recv,
    in_send,
    direct_sem,
    forward_sem,
    forward_send,
    send_sem,
    out_sem,
):
    rows, cols = xv.shape
    size = buf.shape[4]
    heads = cols // HEAD
    width = turned.shape[1]
    positions = spike_raw.shape[2]
    tiles = width // TILE
    parts = positions // size
    spans = positions // rows
    chips = lanes_axis // 2
    slots = stages
    last = stages - 1
    stage = lax.axis_index("pp")
    lane = lax.axis_index("tp")
    core = lax.rem(lane, 2)
    other = 1 - core
    z = lane // 2
    partner = z * 2 + other

    barrier = pltpu.get_barrier_semaphore()

    def ready(to_stage, to_lane):
        pl.semaphore_signal(
            barrier,
            inc=1,
            device_id=at(to_stage, to_lane),
            device_id_type=pl.DeviceIdType.MESH,
        )

    ready(stage, partner)

    @pl.when(stage == 0)
    def _():
        for source in range(stages):
            for over in range(chips):
                ready(source, over * 2 + other)

    @pl.when(stage == 1)
    def _():
        for over in range(lanes_axis):
            ready(0, over)

    @pl.when(stage > 1)
    def _():
        for over in range(chips):
            ready(stage - 1, over * 2 + other)

    ready_from_last = [(last, z * 2 + c) for c in range(2)]
    for c in range(2):

        @pl.when((stage != last) | (core != c))
        def _():
            ready(*ready_from_last[c])

    onward = jnp.where(
        stage == 0,
        2 * chips,
        jnp.where(stage == last, 2 * stages - 1, chips),
    )
    greetings = 1 + chips + onward

    small = [
        pltpu.make_async_copy(scale_ref, scale_v, load_sem.at[2]),
        pltpu.make_async_copy(low_ref, lows.at[core], load_sem.at[3]),
        pltpu.make_async_copy(spike_ref.at[0], spike_raw.at[core], load_sem.at[4]),
    ]
    x_load = pltpu.make_async_copy(x_ref, xv, load_sem.at[0])
    x_load.start()
    for k in range(chips):
        small.append(
            pltpu.make_async_copy(
                gain_ref.at[:, k * 2 * cols : (k + 1) * 2 * cols],
                gain_v.at[k],
                load_sem.at[5 + k],
            )
        )
    for load in small:
        load.start()
    loads = []
    for role, ref in enumerate((wq_ref, wf_ref, wi_ref, wg_ref)):
        load = pltpu.make_async_copy(
            ref.at[0], weights.at[pl.ds(role * cols, cols)], w_sem.at[role]
        )
        load.start()
        loads.append(load)

    sequence = stage // spans
    in_parity = lax.rem(sequence, 2)
    in_slot = (sequence // 2) * parts + lax.rem(stage, spans) * 2

    def farthest_first(send):
        for far in range(chips - 1, 0, -1):

            @pl.when(z + far < chips)
            def _():
                send(z + far)

            @pl.when(z - far >= 0)
            def _():
                send(z - far)

    def to_first(target, half):
        return pltpu.make_async_remote_copy(
            src_ref=xv.at[pl.ds(half * size, size)],
            dst_ref=buf.at[in_slot + half, in_parity, core, z],
            send_sem=in_send.at[target],
            recv_sem=direct_sem.at[in_slot + half, in_parity, z],
            device_id=at(0, target * 2 + other),
            device_id_type=pl.DeviceIdType.MESH,
        )

    def enter(half):
        farthest_first(lambda target: to_first(target, half).start())
        to_first(z, half).start()

    def swap_small(which):
        src, dst = (
            (lows.at[core], lows.at[core])
            if which == 0
            else (spike_raw.at[core], spike_raw.at[core])
        )
        return pltpu.make_async_remote_copy(
            src_ref=src,
            dst_ref=dst,
            send_sem=swap_send.at[1 + which],
            recv_sem=swap_recv.at[tiles + which],
            device_id=at(stage, partner),
            device_id_type=pl.DeviceIdType.MESH,
        )

    def swap_tile(k):
        tile = turned.at[core, pl.ds(pl.multiple_of(k * TILE, TILE), TILE)]
        return pltpu.make_async_remote_copy(
            src_ref=tile,
            dst_ref=tile,
            send_sem=swap_send.at[0],
            recv_sem=swap_recv.at[k],
            device_id=at(stage, partner),
            device_id_type=pl.DeviceIdType.MESH,
        )

    head_of_lane = lax.broadcasted_iota(jnp.int32, (size, cols), 1) // HEAD
    row = lax.broadcasted_iota(jnp.int32, (size, cols), 0)
    tall_row = lax.rem(lax.broadcasted_iota(jnp.int32, (heads * size, size), 0), size)
    tall_col = lax.broadcasted_iota(jnp.int32, (heads * size, size), 1)
    tall_mask = tall_row >= tall_col
    sq_row = lax.broadcasted_iota(jnp.int32, (cols, cols), 0) // HEAD
    sq_col = lax.broadcasted_iota(jnp.int32, (cols, cols), 1) // HEAD
    same_head = sq_row == sq_col
    mean_ones = jnp.where(same_head, 1.0 / HEAD, 0.0).astype(BF16)

    def spread(half):
        for part in range(parts):
            piece = spike_raw[half, :, part * size : (part + 1) * size].T
            wide = jnp.zeros((size, cols), F32)
            for h in range(heads):
                wide = jnp.where(head_of_lane == h, piece[:, h : h + 1], wide)
            spikes[half, part] = jnp.exp(wide)

    x_load.wait()
    pl.semaphore_wait(barrier, greetings)

    @pl.when(in_slot == 0)
    def _():
        enter(0)

    for load in small:
        load.wait()

    @pl.when(stage != 0)
    def _():
        swap_small(0).start()
        swap_small(1).start()

    spread(core)
    for load in loads:
        load.wait()

    def turn(k, carry):
        tile = pl.ds(pl.multiple_of(k * TILE, TILE), TILE)
        for role in range(4):
            turned[core, tile, role * cols : (role + 1) * cols] = weights[
                role * cols : (role + 1) * cols, tile
            ].T

        @pl.when((stage != 0) & (k > 0))
        def _():
            swap_tile(k - 1).start()

        return carry

    lax.fori_loop(0, width // TILE, turn, 0)

    @pl.when(in_slot == 0)
    def _():
        enter(1)

    def whole_wait(ref, sem):
        pltpu.make_async_copy(ref, ref, sem).wait()

    def block(slot, parity, k):
        current = jnp.concatenate(
            [buf[slot, parity, c, k] for c in range(2)], axis=1
        ).astype(F32)
        squares = jnp.sum(current * current, axis=1, keepdims=True)
        return (current * gain_v[k]).astype(BF16), squares

    def gather(slot, parity):
        blocks = [block(slot, parity, k) for k in range(chips)]
        scaled = jnp.concatenate([b[0] for b in blocks], axis=1)
        return scaled, inverse_of(sum(b[1] for b in blocks))

    def inverse_of(squares):
        return lax.rsqrt(squares / width + EPSILON)

    out_gain = jnp.concatenate([scale_v[...]] * heads, axis=1)

    def mix(product, inverse, half, part, memory, stream):
        projected = product * inverse
        query_pre = projected[:, 0 * cols : 1 * cols]
        forget_pre = projected[:, 1 * cols : 2 * cols]
        values = projected[:, 2 * cols : 3 * cols].astype(BF16)
        gate_pre = projected[:, 3 * cols : 4 * cols]

        key_in = (1.0 - lows[half]) * sigmoid(-forget_pre)
        decay = (1.0 - key_in) * spikes[half, part]
        reach = 1
        while reach < size:
            decay = decay * jnp.where(row < reach, 1.0, pltpu.roll(decay, reach, 0))
            reach *= 2
        ending = decay[size - 1 : size, :]
        query_scaled = query_pre * sigmoid(query_pre) * decay
        key_grown = key_in / decay
        key_scaled = key_grown.astype(BF16)
        key_end = (key_grown * ending).astype(BF16)
        query_bf = query_scaled.astype(BF16)
        tall_query = jnp.concatenate(
            [jnp.where(head_of_lane == h, query_scaled, 0.0).astype(BF16) for h in range(heads)],
            axis=0,
        )
        scores = jnp.where(tall_mask, mm(tall_query, key_scaled, NT), 0.0).astype(BF16)
        tall_mixed = mm(scores, values, NN)
        mixed = tall_mixed[0:size]
        for h in range(1, heads):
            mixed = jnp.where(head_of_lane == h, tall_mixed[h * size : (h + 1) * size], mixed)
        if memory is not None:
            mixed = mixed + mm(query_bf, memory.astype(BF16), NT)
        mean_square = mm((mixed * mixed).astype(BF16), mean_ones, NN)
        branch = mixed * lax.rsqrt(mean_square + EPSILON) * out_gain
        branch = branch * (gate_pre * sigmoid(gate_pre))
        return (stream + branch).astype(BF16), (values, key_end, ending)

    def advance(memory, carried):
        values, key_end, ending = carried
        added = jnp.where(same_head, mm(values, key_end, TN), 0.0)
        return added if memory is None else memory * ending + added

    @pl.when(stage == 0)
    def _():
        def to_next(slot, parity, target):
            return pltpu.make_async_remote_copy(
                src_ref=res.at[slot, parity],
                dst_ref=buf.at[slot, parity, core, z],
                send_sem=send_sem.at[slot],
                recv_sem=direct_sem.at[slot, parity, z],
                device_id=at(1, target * 2 + 1 - parity),
                device_id_type=pl.DeviceIdType.MESH,
            )

        def forward(slot, parity):
            half = buf.at[slot, parity, other]
            return pltpu.make_async_remote_copy(
                src_ref=half,
                dst_ref=half,
                send_sem=forward_send.at[slot, parity],
                recv_sem=forward_sem.at[slot, parity],
                device_id=at(stage, partner),
                device_id_type=pl.DeviceIdType.MESH,
            )

        def pass_on(slot, parity):
            for k in range(chips):
                whole_wait(buf.at[slot, parity, other, k], direct_sem.at[slot, parity, k])
            forward(slot, parity).start()

        def finish(slot, parity, part, product, inverse, memory):
            stream = buf[slot, parity, core, z].astype(F32)
            result, carried = mix(product, inverse, core, part, memory, stream)
            res[slot, parity] = result
            farthest_first(lambda target: to_next(slot, parity, target).start())
            to_next(slot, parity, z).start()
            state[parity] = advance(memory, carried)

        pass_on(0, 0)

        def single(parity, carry):
            whole_wait(buf.at[0, parity, core], forward_sem.at[0, parity])
            scaled, inverse = gather(0, parity)
            product = mm(scaled, turned[core], NN)

            @pl.when(parity == 0)
            def _():
                pass_on(0, 1)

            @pl.when(parity == 1)
            def _():
                pass_on(1, 0)
                pass_on(1, 1)

            finish(0, parity, 0, product, inverse, None)
            return carry

        lax.fori_loop(0, 2, single, 0)

        def step(slot, carry):
            part = lax.rem(slot, parts)
            for parity in range(2):
                whole_wait(buf.at[slot, parity, core], forward_sem.at[slot, parity])
            both = [gather(slot, parity) for parity in range(2)]
            product = mm(jnp.concatenate([b[0] for b in both], axis=0), turned[core], NN)

            @pl.when(slot + 1 < slots)
            def _():
                pass_on(slot + 1, 0)
                pass_on(slot + 1, 1)

            for parity in range(2):
                memory = jnp.where(part == 0, 0.0, state[parity])
                own = product[parity * size : (parity + 1) * size]
                finish(slot, parity, part, own, both[parity][1], memory)
            return carry

        lax.fori_loop(1, slots, step, 0)

        def drain(slot, carry):
            for parity in range(2):
                forward(slot, parity).wait_send()
            whole_wait(buf.at[slot, 0], send_sem.at[slot])
            return carry

        lax.fori_loop(0, slots, drain, 0)

    @pl.when(stage != 0)
    def _():
        swap_tile(tiles - 1).start()
        swap_small(0).wait_recv()
        swap_small(1).wait_recv()
        spread(other)
        for k in range(tiles):
            whole_wait(turned.at[other, pl.ds(k * TILE, TILE)], swap_recv.at[k])
            for half in range(2):
                if k == SENT_AFTER[half]:

                    @pl.when(in_slot != 0)
                    def _():
                        enter(half)

        parity = lax.rem(core + stage, 2)
        upper = z // ((chips + 1) // 2)

        def to_next(slot, target):
            return pltpu.make_async_remote_copy(
                src_ref=res.at[slot],
                dst_ref=buf.at[slot, parity, :, z],
                send_sem=send_sem.at[slot],
                recv_sem=direct_sem.at[slot, parity, z],
                device_id=at(lax.rem(stage + 1, stages), target * 2 + other),
                device_id_type=pl.DeviceIdType.MESH,
            )

        def owner(slot):
            part = lax.rem(slot, parts)
            return ((slot // parts) * 2 + parity) * spans + part // 2

        def place(slot):
            start = pl.multiple_of(lax.rem(slot, 2) * size, size)
            return out_ref.at[pl.ds(start, size)]

        def out_copy(slot, half):
            return pltpu.make_async_remote_copy(
                src_ref=res.at[slot, half],
                dst_ref=place(slot),
                send_sem=send_sem.at[slot],
                recv_sem=out_sem,
                device_id=at(owner(slot), z * 2 + half),
                device_id_type=pl.DeviceIdType.MESH,
            )

        def stays(slot, half):
            return (owner(slot) == stage) & (core == half)

        def step(slot, carry):
            part = lax.rem(slot, parts)
            squares, products = 0.0, [0.0, 0.0]
            for j in range(chips):
                k = upper * j + (1 - upper) * (chips - 1 - j)
                whole_wait(buf.at[slot, parity, :, k], direct_sem.at[slot, parity, k])
                scaled, added = block(slot, parity, k)
                squares = squares + added
                span = pl.ds(pl.multiple_of(k * 2 * cols, 2 * cols), 2 * cols)
                for half in range(2):
                    products[half] = products[half] + mm(scaled, turned[half, span], NN)
            inverse = inverse_of(squares)
            kept = []
            for half in range(2):
                product = products[half]
                memory = jnp.where(part == 0, 0.0, state[half])
                stream = buf[slot, parity, half, z].astype(F32)
                result, carried = mix(product, inverse, half, part, memory, stream)
                res[slot, half] = result
                kept.append((memory, carried))

            @pl.when(stage != last)
            def _():
                farthest_first(lambda target: to_next(slot, target).start())
                to_next(slot, z).start()

            for half in range(2):

                @pl.when((stage == last) & ~stays(slot, half))
                def _():
                    out_copy(slot, half).start()

                @pl.when((stage == last) & stays(slot, half))
                def _():
                    pltpu.make_async_copy(res.at[slot, half], place(slot), out_sem).start()

            for half in range(2):
                memory, carried = kept[half]
                state[half] = advance(memory, carried)
            return carry

        lax.fori_loop(0, slots, step, 0)

        def drain(slot, carry):
            @pl.when(stage != last)
            def _():
                whole_wait(buf.at[slot, 0], send_sem.at[slot])

            for half in range(2):

                @pl.when((stage == last) & ~stays(slot, half))
                def _():
                    out_copy(slot, half).wait_send()

            return carry

        lax.fori_loop(0, slots, drain, 0)
        whole_wait(turned.at[core], swap_send.at[0])
        swap_small(0).wait_send()
        swap_small(1).wait_send()

    for target in range(chips):
        whole_wait(xv, in_send.at[target])

    whole_wait(out_ref, out_sem)


def solution(mesh):
    stages = mesh.shape["pp"]
    lanes_axis = mesh.shape["tp"]
    chips = lanes_axis // 2

    def step(x, gain, wq, wf, wi, wg, low, spike, scale):
        rows, cols = x.shape
        width = gain.shape[1]
        positions = spike.shape[1]
        heads = cols // HEAD
        size = rows // 2
        parts = positions // size
        vmem = pl.BlockSpec(memory_space=pltpu.VMEM)
        hbm = pl.BlockSpec(memory_space=pl.ANY)
        dma = pltpu.SemaphoreType.DMA
        return pl.pallas_call(
            functools.partial(kernel, stages, lanes_axis),
            out_shape=jax.ShapeDtypeStruct((rows, cols), BF16),
            in_specs=[hbm] * 9,
            out_specs=vmem,
            scratch_shapes=[
                pltpu.VMEM((rows, cols), BF16),
                pltpu.VMEM((chips, 1, 2 * cols), F32),
                pltpu.VMEM(scale.shape, F32),
                pltpu.VMEM((2, 1, cols), F32),
                pltpu.VMEM((2, heads, positions), F32),
                pltpu.VMEM((4 * cols, width), BF16),
                pltpu.VMEM((2, width, 4 * cols), BF16),
                pltpu.VMEM((stages, 2, 2, chips, size, cols), BF16),
                pltpu.VMEM((stages, 2, size, cols), BF16),
                pltpu.VMEM((2, parts, size, cols), F32),
                pltpu.VMEM((2, cols, cols), F32),
                dma((5 + chips,)),
                dma((4,)),
                dma((3,)),
                dma((width // TILE + 2,)),
                dma((chips,)),
                dma((stages, 2, chips)),
                dma((stages, 2)),
                dma((stages, 2)),
                dma((stages,)),
                dma,
            ],
            compiler_params=pltpu.CompilerParams(
                collective_id=0, has_side_effects=True, vmem_limit_bytes=GRANT
            ),
        )(
            *[
                pltpu.with_memory_space_constraint(v, pltpu.HBM)
                for v in (x, gain, wq, wf, wi, wg, low, spike.transpose(0, 2, 1), scale)
            ]
        )

    in_specs = (
        P("pp", "tp"),
        P("pp", None),
        P("pp", "tp", None),
        P("pp", "tp", None),
        P("pp", "tp", None),
        P("pp", "tp", None),
        P("pp", "tp"),
        P("pp", None, "tp"),
        P("pp", None),
    )
    return jax.shard_map(
        step, mesh=mesh, in_specs=in_specs, out_specs=P("pp", "tp"), check_vma=False
    )
```

```python
import functools

import jax
import jax.numpy as jnp
from jax import lax
from jax.experimental import pallas as pl
from jax.experimental.pallas import tpu as pltpu
from jax.sharding import PartitionSpec as P

HEAD = 64
TILE = 256
EPSILON = 1e-06
GRANT = 40 * 2**20
SENT_AFTER = (1, 4)
F32 = jnp.float32
BF16 = jnp.bfloat16
NT = (((1,), (1,)), ((), ()))
NN = (((1,), (0,)), ((), ()))
TN = (((0,), (0,)), ((), ()))


def mm(a, b, dims):
    return lax.dot_general(a, b, dims, preferred_element_type=F32)


def sigmoid(v):
    return 1.0 / (1.0 + jnp.exp(-v))


def at(stage, lane):
    return {"pp": stage, "tp": lane}


def kernel(
    stages,
    lanes_axis,
    x_ref,
    gain_ref,
    wq_ref,
    wf_ref,
    wi_ref,
    wg_ref,
    low_ref,
    spike_ref,
    scale_ref,
    out_ref,
    xv,
    gain_v,
    scale_v,
    lows,
    spike_raw,
    weights,
    turned,
    buf,
    res,
    spikes,
    state,
    load_sem,
    w_sem,
    swap_send,
    swap_recv,
    in_send,
    direct_sem,
    forward_sem,
    forward_send,
    send_sem,
    out_sem,
):
    rows, cols = xv.shape
    size = buf.shape[4]
    heads = cols // HEAD
    width = turned.shape[1]
    positions = spike_raw.shape[2]
    tiles = width // TILE
    parts = positions // size
    spans = positions // rows
    chips = lanes_axis // 2
    slots = stages
    last = stages - 1
    stage = lax.axis_index("pp")
    lane = lax.axis_index("tp")
    core = lax.rem(lane, 2)
    other = 1 - core
    z = lane // 2
    partner = z * 2 + other

    barrier = pltpu.get_barrier_semaphore()

    def ready(to_stage, to_lane):
        pl.semaphore_signal(
            barrier,
            inc=1,
            device_id=at(to_stage, to_lane),
            device_id_type=pl.DeviceIdType.MESH,
        )

    ready(stage, partner)

    @pl.when(stage == 0)
    def _():
        for source in range(stages):
            for over in range(chips):
                ready(source, over * 2 + other)

    @pl.when(stage == 1)
    def _():
        for over in range(lanes_axis):
            ready(0, over)

    @pl.when(stage > 1)
    def _():
        for over in range(chips):
            ready(stage - 1, over * 2 + other)

    ready_from_last = [(last, z * 2 + c) for c in range(2)]
    for c in range(2):

        @pl.when((stage != last) | (core != c))
        def _():
            ready(*ready_from_last[c])

    onward = jnp.where(
        stage == 0,
        2 * chips,
        jnp.where(stage == last, 2 * stages - 1, chips),
    )
    greetings = 1 + chips + onward

    small = [
        pltpu.make_async_copy(scale_ref, scale_v, load_sem.at[2]),
        pltpu.make_async_copy(low_ref, lows.at[core], load_sem.at[3]),
        pltpu.make_async_copy(spike_ref.at[0], spike_raw.at[core], load_sem.at[4]),
    ]
    x_load = pltpu.make_async_copy(x_ref, xv, load_sem.at[0])
    x_load.start()
    for k in range(chips):
        small.append(
            pltpu.make_async_copy(
                gain_ref.at[:, k * 2 * cols : (k + 1) * 2 * cols],
                gain_v.at[k],
                load_sem.at[5 + k],
            )
        )
    for load in small:
        load.start()
    loads = []
    for role, ref in enumerate((wq_ref, wf_ref, wi_ref, wg_ref)):
        load = pltpu.make_async_copy(
            ref.at[0], weights.at[pl.ds(role * cols, cols)], w_sem.at[role]
        )
        load.start()
        loads.append(load)

    sequence = stage // spans
    in_parity = lax.rem(sequence, 2)
    in_slot = (sequence // 2) * parts + lax.rem(stage, spans) * 2

    def farthest_first(send):
        for far in range(chips - 1, 0, -1):

            @pl.when(z + far < chips)
            def _():
                send(z + far)

            @pl.when(z - far >= 0)
            def _():
                send(z - far)

    def own_first(send):
        send(z)
        farthest_first(send)

    def to_first(target, half):
        return pltpu.make_async_remote_copy(
            src_ref=xv.at[pl.ds(half * size, size)],
            dst_ref=buf.at[in_slot + half, in_parity, core, z],
            send_sem=in_send.at[target],
            recv_sem=direct_sem.at[in_slot + half, in_parity, z],
            device_id=at(0, target * 2 + other),
            device_id_type=pl.DeviceIdType.MESH,
        )

    def enter(half):
        farthest_first(lambda target: to_first(target, half).start())
        to_first(z, half).start()

    def swap_small(which):
        src, dst = (
            (lows.at[core], lows.at[core])
            if which == 0
            else (spike_raw.at[core], spike_raw.at[core])
        )
        return pltpu.make_async_remote_copy(
            src_ref=src,
            dst_ref=dst,
            send_sem=swap_send.at[1 + which],
            recv_sem=swap_recv.at[tiles + which],
            device_id=at(stage, partner),
            device_id_type=pl.DeviceIdType.MESH,
        )

    def swap_tile(k):
        tile = turned.at[core, pl.ds(pl.multiple_of(k * TILE, TILE), TILE)]
        return pltpu.make_async_remote_copy(
            src_ref=tile,
            dst_ref=tile,
            send_sem=swap_send.at[0],
            recv_sem=swap_recv.at[k],
            device_id=at(stage, partner),
            device_id_type=pl.DeviceIdType.MESH,
        )

    head_of_lane = lax.broadcasted_iota(jnp.int32, (size, cols), 1) // HEAD
    row = lax.broadcasted_iota(jnp.int32, (size, cols), 0)
    tall_row = lax.rem(lax.broadcasted_iota(jnp.int32, (heads * size, size), 0), size)
    tall_col = lax.broadcasted_iota(jnp.int32, (heads * size, size), 1)
    tall_mask = tall_row >= tall_col
    sq_row = lax.broadcasted_iota(jnp.int32, (cols, cols), 0) // HEAD
    sq_col = lax.broadcasted_iota(jnp.int32, (cols, cols), 1) // HEAD
    same_head = sq_row == sq_col
    lane_head = lax.broadcasted_iota(jnp.int32, (HEAD, cols), 1) // HEAD
    mean_ones = jnp.where(same_head, 1.0 / HEAD, 0.0).astype(BF16)

    def spread(half):
        for part in range(parts):
            piece = spike_raw[half, :, part * size : (part + 1) * size].T
            wide = jnp.zeros((size, cols), F32)
            for h in range(heads):
                wide = jnp.where(head_of_lane == h, piece[:, h : h + 1], wide)
            spikes[half, part] = jnp.exp(wide)

    x_load.wait()
    pl.semaphore_wait(barrier, greetings)

    @pl.when(in_slot == 0)
    def _():
        enter(0)

    for load in small:
        load.wait()

    @pl.when(stage != 0)
    def _():
        swap_small(0).start()
        swap_small(1).start()

    spread(core)
    for load in loads:
        load.wait()

    def turn(k, carry):
        tile = pl.ds(pl.multiple_of(k * TILE, TILE), TILE)
        for role in range(4):
            turned[core, tile, role * cols : (role + 1) * cols] = weights[
                role * cols : (role + 1) * cols, tile
            ].T

        @pl.when((stage != 0) & (k > 0))
        def _():
            swap_tile(k - 1).start()

        return carry

    lax.fori_loop(0, width // TILE, turn, 0)

    @pl.when(in_slot == 0)
    def _():
        enter(1)

    def whole_wait(ref, sem):
        pltpu.make_async_copy(ref, ref, sem).wait()

    def block(slot, parity, k):
        current = jnp.concatenate(
            [buf[slot, parity, c, k] for c in range(2)], axis=1
        ).astype(F32)
        squares = jnp.sum(current * current, axis=1, keepdims=True)
        return (current * gain_v[k]).astype(BF16), squares

    def gather(slot, parity):
        blocks = [block(slot, parity, k) for k in range(chips)]
        scaled = jnp.concatenate([b[0] for b in blocks], axis=1)
        return scaled, inverse_of(sum(b[1] for b in blocks))

    def inverse_of(squares):
        return lax.rsqrt(squares / width + EPSILON)

    out_gain = jnp.concatenate([scale_v[...]] * heads, axis=1)

    def mix(product, inverse, half, part, memory, stream):
        projected = product * inverse
        query_pre = projected[:, 0 * cols : 1 * cols]
        forget_pre = projected[:, 1 * cols : 2 * cols]
        values = projected[:, 2 * cols : 3 * cols].astype(BF16)
        gate_pre = projected[:, 3 * cols : 4 * cols]

        key_in = (1.0 - lows[half]) * sigmoid(-forget_pre)
        decay = (1.0 - key_in) * spikes[half, part]
        reach = 1
        while reach < size:
            decay = decay * jnp.where(row < reach, 1.0, pltpu.roll(decay, reach, 0))
            reach *= 2
        ending = decay[size - 1 : size, :]
        query_scaled = query_pre * sigmoid(query_pre) * decay
        key_grown = key_in / decay
        key_scaled = key_grown.astype(BF16)
        key_end = (key_grown * ending).astype(BF16)
        query_bf = query_scaled.astype(BF16)
        tall_query = jnp.concatenate(
            [jnp.where(head_of_lane == h, query_scaled, 0.0).astype(BF16) for h in range(heads)],
            axis=0,
        )
        scores = jnp.where(tall_mask, mm(tall_query, key_scaled, NT), 0.0).astype(BF16)
        tall_mixed = mm(scores, values, NN)
        mixed = tall_mixed[0:size]
        for h in range(1, heads):
            mixed = jnp.where(head_of_lane == h, tall_mixed[h * size : (h + 1) * size], mixed)
        if memory is not None:
            tiled = jnp.concatenate([memory.astype(BF16)] * heads, axis=0)
            mixed = mixed + mm(query_bf, jnp.where(same_head, tiled, jnp.zeros_like(tiled)), NT)
        mean_square = mm((mixed * mixed).astype(BF16), mean_ones, NN)
        branch = mixed * lax.rsqrt(mean_square + EPSILON) * out_gain
        branch = branch * (gate_pre * sigmoid(gate_pre))
        return (stream + branch).astype(BF16), (values, key_end, ending)

    def advance(memory, carried):
        values, key_end, ending = carried
        spread_out = mm(values, key_end, TN)
        added = spread_out[0:HEAD]
        for h in range(1, heads):
            added = jnp.where(lane_head == h, spread_out[h * HEAD : (h + 1) * HEAD], added)
        return added if memory is None else memory * ending + added

    @pl.when(stage == 0)
    def _():
        def to_next(slot, parity, target):
            return pltpu.make_async_remote_copy(
                src_ref=res.at[slot, parity],
                dst_ref=buf.at[slot, parity, core, z],
                send_sem=send_sem.at[slot, parity],
                recv_sem=direct_sem.at[slot, parity, z],
                device_id=at(1, target * 2 + 1 - parity),
                device_id_type=pl.DeviceIdType.MESH,
            )

        def forward(slot, parity):
            half = buf.at[slot, parity, other]
            return pltpu.make_async_remote_copy(
                src_ref=half,
                dst_ref=half,
                send_sem=forward_send.at[slot, parity],
                recv_sem=forward_sem.at[slot, parity],
                device_id=at(stage, partner),
                device_id_type=pl.DeviceIdType.MESH,
            )

        def pass_on(slot, parity):
            for k in range(chips):
                whole_wait(buf.at[slot, parity, other, k], direct_sem.at[slot, parity, k])
            forward(slot, parity).start()

        def sent(slot):
            for parity in range(2):
                whole_wait(buf.at[slot, parity, core], send_sem.at[slot, parity])

        def turn_of(slot, parity):
            @pl.when((slot > 0) & (parity == 0))
            def _():
                sent(slot - 1)

        def finish(slot, parity, part, product, inverse, memory):
            stream = buf[slot, parity, core, z].astype(F32)
            result, carried = mix(product, inverse, core, part, memory, stream)
            res[slot, parity] = result
            turn_of(slot, parity)
            own_first(lambda target: to_next(slot, parity, target).start())
            state[parity] = advance(memory, carried)

        pass_on(0, 0)

        def single(parity, carry):
            whole_wait(buf.at[0, parity, core], forward_sem.at[0, parity])
            scaled, inverse = gather(0, parity)
            product = mm(scaled, turned[core], NN)

            @pl.when(parity == 0)
            def _():
                pass_on(0, 1)

            @pl.when(parity == 1)
            def _():
                pass_on(1, 0)
                pass_on(1, 1)

            finish(0, parity, 0, product, inverse, None)
            return carry

        lax.fori_loop(0, 2, single, 0)

        def step(slot, carry):
            part = lax.rem(slot, parts)
            for parity in range(2):
                whole_wait(buf.at[slot, parity, core], forward_sem.at[slot, parity])
            both = [gather(slot, parity) for parity in range(2)]
            product = mm(jnp.concatenate([b[0] for b in both], axis=0), turned[core], NN)

            @pl.when(slot + 1 < slots)
            def _():
                pass_on(slot + 1, 0)
                pass_on(slot + 1, 1)

            for parity in range(2):
                memory = jnp.where(part == 0, 0.0, state[parity])
                own = product[parity * size : (parity + 1) * size]
                finish(slot, parity, part, own, both[parity][1], memory)
            return carry

        lax.fori_loop(1, slots, step, 0)

        def drain(slot, carry):
            for parity in range(2):
                forward(slot, parity).wait_send()
            return carry

        lax.fori_loop(0, slots, drain, 0)
        sent(slots - 1)

    @pl.when(stage != 0)
    def _():
        swap_tile(tiles - 1).start()
        swap_small(0).wait_recv()
        swap_small(1).wait_recv()
        spread(other)
        for k in range(tiles):
            whole_wait(turned.at[other, pl.ds(k * TILE, TILE)], swap_recv.at[k])
            for half in range(2):
                if k == SENT_AFTER[half]:

                    @pl.when(in_slot != 0)
                    def _():
                        enter(half)

        parity = lax.rem(core + stage, 2)
        upper = z // ((chips + 1) // 2)

        def to_next(slot, target):
            return pltpu.make_async_remote_copy(
                src_ref=res.at[slot],
                dst_ref=buf.at[slot, parity, :, z],
                send_sem=send_sem.at[slot, 0],
                recv_sem=direct_sem.at[slot, parity, z],
                device_id=at(lax.rem(stage + 1, stages), target * 2 + other),
                device_id_type=pl.DeviceIdType.MESH,
            )

        def owner(slot):
            part = lax.rem(slot, parts)
            return ((slot // parts) * 2 + parity) * spans + part // 2

        def place(slot):
            start = pl.multiple_of(lax.rem(slot, 2) * size, size)
            return out_ref.at[pl.ds(start, size)]

        def out_copy(slot, half):
            return pltpu.make_async_remote_copy(
                src_ref=res.at[slot, half],
                dst_ref=place(slot),
                send_sem=send_sem.at[slot, half],
                recv_sem=out_sem,
                device_id=at(owner(slot), z * 2 + half),
                device_id_type=pl.DeviceIdType.MESH,
            )

        def stays(slot, half):
            return (owner(slot) == stage) & (core == half)

        def step(slot, carry):
            part = lax.rem(slot, parts)
            squares, products = 0.0, [0.0, 0.0]
            for j in range(chips):
                k = upper * j + (1 - upper) * (chips - 1 - j)
                whole_wait(buf.at[slot, parity, :, k], direct_sem.at[slot, parity, k])
                scaled, added = block(slot, parity, k)
                squares = squares + added
                span = pl.ds(pl.multiple_of(k * 2 * cols, 2 * cols), 2 * cols)
                for half in range(2):
                    products[half] = products[half] + mm(scaled, turned[half, span], NN)
            inverse = inverse_of(squares)
            kept = []
            for half in range(2):
                product = products[half]
                memory = jnp.where(part == 0, 0.0, state[half])
                stream = buf[slot, parity, half, z].astype(F32)
                result, carried = mix(product, inverse, half, part, memory, stream)
                res[slot, half] = result
                kept.append((memory, carried))

            @pl.when(stage != last)
            def _():
                own_first(lambda target: to_next(slot, target).start())

            for half in range(2):

                @pl.when((stage == last) & ~stays(slot, half))
                def _():
                    out_copy(slot, half).start()

                @pl.when((stage == last) & stays(slot, half))
                def _():
                    pltpu.make_async_copy(res.at[slot, half], place(slot), out_sem).start()

            for half in range(2):
                memory, carried = kept[half]
                state[half] = advance(memory, carried)
            return carry

        lax.fori_loop(0, slots, step, 0)

        def drain(slot, carry):
            @pl.when(stage != last)
            def _():
                whole_wait(buf.at[slot, 0], send_sem.at[slot, 0])

            for half in range(2):

                @pl.when((stage == last) & ~stays(slot, half))
                def _():
                    out_copy(slot, half).wait_send()

            return carry

        lax.fori_loop(0, slots, drain, 0)
        whole_wait(turned.at[core], swap_send.at[0])
        swap_small(0).wait_send()
        swap_small(1).wait_send()

    for target in range(chips):
        whole_wait(xv, in_send.at[target])

    whole_wait(out_ref, out_sem)


def solution(mesh):
    stages = mesh.shape["pp"]
    lanes_axis = mesh.shape["tp"]
    chips = lanes_axis // 2

    def step(x, gain, wq, wf, wi, wg, low, spike, scale):
        rows, cols = x.shape
        width = gain.shape[1]
        positions = spike.shape[1]
        heads = cols // HEAD
        size = rows // 2
        parts = positions // size
        vmem = pl.BlockSpec(memory_space=pltpu.VMEM)
        hbm = pl.BlockSpec(memory_space=pl.ANY)
        dma = pltpu.SemaphoreType.DMA
        return pl.pallas_call(
            functools.partial(kernel, stages, lanes_axis),
            out_shape=jax.ShapeDtypeStruct((rows, cols), BF16),
            in_specs=[hbm] * 9,
            out_specs=vmem,
            scratch_shapes=[
                pltpu.VMEM((rows, cols), BF16),
                pltpu.VMEM((chips, 1, 2 * cols), F32),
                pltpu.VMEM(scale.shape, F32),
                pltpu.VMEM((2, 1, cols), F32),
                pltpu.VMEM((2, heads, positions), F32),
                pltpu.VMEM((4 * cols, width), BF16),
                pltpu.VMEM((2, width, 4 * cols), BF16),
                pltpu.VMEM((stages, 2, 2, chips, size, cols), BF16),
                pltpu.VMEM((stages, 2, size, cols), BF16),
                pltpu.VMEM((2, parts, size, cols), F32),
                pltpu.VMEM((2, HEAD, cols), F32),
                dma((5 + chips,)),
                dma((4,)),
                dma((3,)),
                dma((width // TILE + 2,)),
                dma((chips,)),
                dma((stages, 2, chips)),
                dma((stages, 2)),
                dma((stages, 2)),
                dma((stages, 2)),
                dma,
            ],
            compiler_params=pltpu.CompilerParams(
                collective_id=0, has_side_effects=True, vmem_limit_bytes=GRANT
            ),
        )(
            *[
                pltpu.with_memory_space_constraint(v, pltpu.HBM)
                for v in (x, gain, wq, wf, wi, wg, low, spike.transpose(0, 2, 1), scale)
            ]
        )

    in_specs = (
        P("pp", "tp"),
        P("pp", None),
        P("pp", "tp", None),
        P("pp", "tp", None),
        P("pp", "tp", None),
        P("pp", "tp", None),
        P("pp", "tp"),
        P("pp", None, "tp"),
        P("pp", None),
    )
    return jax.shard_map(
        step, mesh=mesh, in_specs=in_specs, out_specs=P("pp", "tp"), check_vma=False
    )
```

```python
import functools

import jax
import jax.numpy as jnp
from jax import lax
from jax.experimental import pallas as pl
from jax.experimental.pallas import tpu as pltpu
from jax.sharding import PartitionSpec as P

HEAD = 64
TILE = 256
EPSILON = 1e-06
GRANT = 40 * 2**20
F32 = jnp.float32
BF16 = jnp.bfloat16
NT = (((1,), (1,)), ((), ()))
NN = (((1,), (0,)), ((), ()))
TN = (((0,), (0,)), ((), ()))


def mm(a, b, dims):
    return lax.dot_general(a, b, dims, preferred_element_type=F32)


def sigmoid(v):
    return 1.0 / (1.0 + jnp.exp(-v))


def at(stage, lane):
    return {"pp": stage, "tp": lane}


def kernel(
    stages,
    lanes_axis,
    x_ref,
    gain_ref,
    wq_ref,
    wf_ref,
    wi_ref,
    wg_ref,
    low_ref,
    spike_ref,
    scale_ref,
    out_ref,
    xv,
    gain_v,
    scale_v,
    lows,
    spike_raw,
    weights,
    turned,
    buf,
    res,
    spikes,
    state,
    load_sem,
    w_sem,
    swap_send,
    swap_recv,
    in_send,
    direct_sem,
    forward_sem,
    forward_send,
    send_sem,
    out_sem,
):
    rows, cols = xv.shape
    size = buf.shape[4]
    heads = cols // HEAD
    width = turned.shape[1]
    positions = spike_raw.shape[2]
    tiles = width // TILE
    groups = tiles // 3 + 1
    parts = positions // size
    spans = positions // rows
    chips = lanes_axis // 2
    slots = stages
    last = stages - 1
    stage = lax.axis_index("pp")
    lane = lax.axis_index("tp")
    core = lax.rem(lane, 2)
    other = 1 - core
    z = lane // 2
    partner = z * 2 + other

    barrier = pltpu.get_barrier_semaphore()

    def ready(to_stage, to_lane):
        pl.semaphore_signal(
            barrier,
            inc=1,
            device_id=at(to_stage, to_lane),
            device_id_type=pl.DeviceIdType.MESH,
        )

    ready(stage, partner)

    @pl.when(stage == 0)
    def _():
        for source in range(stages):
            for over in range(chips):
                ready(source, over * 2 + other)

    @pl.when(stage == 1)
    def _():
        for over in range(lanes_axis):
            ready(0, over)

    @pl.when(stage > 1)
    def _():
        for over in range(chips):
            ready(stage - 1, over * 2 + other)

    ready_from_last = [(last, z * 2 + c) for c in range(2)]
    for c in range(2):

        @pl.when((stage != last) | (core != c))
        def _():
            ready(*ready_from_last[c])

    onward = jnp.where(
        stage == 0,
        2 * chips,
        jnp.where(stage == last, 2 * stages - 1, chips),
    )
    greetings = 1 + chips + onward

    small = [
        pltpu.make_async_copy(scale_ref, scale_v, load_sem.at[2]),
        pltpu.make_async_copy(low_ref, lows.at[core], load_sem.at[3]),
        pltpu.make_async_copy(spike_ref.at[0], spike_raw.at[core], load_sem.at[4]),
    ]
    x_load = pltpu.make_async_copy(x_ref, xv, load_sem.at[0])
    x_load.start()
    for k in range(chips):
        pltpu.make_async_copy(
            gain_ref.at[:, k * 2 * cols : (k + 1) * 2 * cols], gain_v.at[k], load_sem.at[1]
        ).start()
    for load in small:
        load.start()
    for role, ref in enumerate((wq_ref, wf_ref, wi_ref, wg_ref)):
        pltpu.make_async_copy(
            ref.at[0], weights.at[pl.ds(role * cols, cols)], w_sem
        ).start()

    sequence = stage // spans
    in_parity = lax.rem(sequence, 2)
    in_slot = (sequence // 2) * parts + lax.rem(stage, spans) * 2

    def whole_wait(ref, sem):
        pltpu.make_async_copy(ref, ref, sem).wait()

    def farthest_first(send):
        for far in range(chips - 1, 0, -1):

            @pl.when(z + far < chips)
            def _():
                send(z + far)

            @pl.when(z - far >= 0)
            def _():
                send(z - far)

    def own_first(send):
        send(z)
        farthest_first(send)

    def to_first(target, half):
        return pltpu.make_async_remote_copy(
            src_ref=xv.at[pl.ds(half * size, size)],
            dst_ref=buf.at[in_slot + half, in_parity, core, z],
            send_sem=in_send,
            recv_sem=direct_sem.at[in_slot + half, in_parity],
            device_id=at(0, target * 2 + other),
            device_id_type=pl.DeviceIdType.MESH,
        )

    def enter(half):
        farthest_first(lambda target: to_first(target, half).start())
        to_first(z, half).start()

    def swap_small(which):
        src, dst = (
            (lows.at[core], lows.at[core])
            if which == 0
            else (spike_raw.at[core], spike_raw.at[core])
        )
        return pltpu.make_async_remote_copy(
            src_ref=src,
            dst_ref=dst,
            send_sem=swap_send.at[1 + which],
            recv_sem=swap_recv.at[groups + which],
            device_id=at(stage, partner),
            device_id_type=pl.DeviceIdType.MESH,
        )

    def swap_tile(k):
        tile = turned.at[core, pl.ds(pl.multiple_of(k * TILE, TILE), TILE)]
        return pltpu.make_async_remote_copy(
            src_ref=tile,
            dst_ref=tile,
            send_sem=swap_send.at[0],
            recv_sem=swap_recv.at[(k + 1) // 3],
            device_id=at(stage, partner),
            device_id_type=pl.DeviceIdType.MESH,
        )

    head_of_lane = lax.broadcasted_iota(jnp.int32, (size, cols), 1) // HEAD
    row = lax.broadcasted_iota(jnp.int32, (size, cols), 0)
    tall_row = lax.rem(lax.broadcasted_iota(jnp.int32, (heads * size, size), 0), size)
    tall_col = lax.broadcasted_iota(jnp.int32, (heads * size, size), 1)
    tall_mask = tall_row >= tall_col
    sq_row = lax.broadcasted_iota(jnp.int32, (cols, cols), 0) // HEAD
    sq_col = lax.broadcasted_iota(jnp.int32, (cols, cols), 1) // HEAD
    same_head = sq_row == sq_col
    lane_head = lax.broadcasted_iota(jnp.int32, (HEAD, cols), 1) // HEAD
    mean_ones = jnp.where(same_head, 1.0 / HEAD, 0.0).astype(BF16)

    def spread(half):
        for part in range(parts):
            piece = spike_raw[half, :, part * size : (part + 1) * size].T
            wide = jnp.zeros((size, cols), F32)
            for h in range(heads):
                wide = jnp.where(head_of_lane == h, piece[:, h : h + 1], wide)
            spikes[half, part] = jnp.exp(wide)

    x_load.wait()
    pl.semaphore_wait(barrier, greetings)

    @pl.when(in_slot == 0)
    def _():
        enter(0)

    for load in small:
        load.wait()
    whole_wait(gain_v, load_sem.at[1])

    @pl.when(stage != 0)
    def _():
        swap_small(0).start()
        swap_small(1).start()

    spread(core)
    whole_wait(weights, w_sem)

    def turn(k, carry):
        tile = pl.ds(pl.multiple_of(k * TILE, TILE), TILE)
        for role in range(4):
            turned[core, tile, role * cols : (role + 1) * cols] = weights[
                role * cols : (role + 1) * cols, tile
            ].T

        @pl.when((stage != 0) & (k > 0))
        def _():
            swap_tile(k - 1).start()

        return carry

    lax.fori_loop(0, width // TILE, turn, 0)

    @pl.when(in_slot == 0)
    def _():
        enter(1)

    def block(slot, parity, k):
        current = jnp.concatenate(
            [buf[slot, parity, c, k] for c in range(2)], axis=1
        ).astype(F32)
        squares = jnp.sum(current * current, axis=1, keepdims=True)
        return (current * gain_v[k]).astype(BF16), squares

    def gather(slot, parity):
        blocks = [block(slot, parity, k) for k in range(chips)]
        scaled = jnp.concatenate([b[0] for b in blocks], axis=1)
        return scaled, inverse_of(sum(b[1] for b in blocks))

    def inverse_of(squares):
        return lax.rsqrt(squares / width + EPSILON)

    out_gain = jnp.concatenate([scale_v[...]] * heads, axis=1)

    def mix(product, inverse, half, part, memory, stream):
        projected = product * inverse
        query_pre = projected[:, 0 * cols : 1 * cols]
        forget_pre = projected[:, 1 * cols : 2 * cols]
        values = projected[:, 2 * cols : 3 * cols].astype(BF16)
        gate_pre = projected[:, 3 * cols : 4 * cols]

        key_in = (1.0 - lows[half]) * sigmoid(-forget_pre)
        decay = (1.0 - key_in) * spikes[half, part]
        reach = 1
        while reach < size:
            decay = decay * jnp.where(row < reach, 1.0, pltpu.roll(decay, reach, 0))
            reach *= 2
        ending = decay[size - 1 : size, :]
        query_scaled = query_pre * sigmoid(query_pre) * decay
        key_grown = key_in / decay
        key_scaled = key_grown.astype(BF16)
        key_end = (key_grown * ending).astype(BF16)
        query_bf = query_scaled.astype(BF16)
        tall_query = jnp.concatenate(
            [jnp.where(head_of_lane == h, query_scaled, 0.0).astype(BF16) for h in range(heads)],
            axis=0,
        )
        scores = jnp.where(tall_mask, mm(tall_query, key_scaled, NT), 0.0).astype(BF16)
        tall_mixed = mm(scores, values, NN)
        mixed = tall_mixed[0:size]
        for h in range(1, heads):
            mixed = jnp.where(head_of_lane == h, tall_mixed[h * size : (h + 1) * size], mixed)
        if memory is not None:
            tiled = jnp.concatenate([memory.astype(BF16)] * heads, axis=0)
            mixed = mixed + mm(query_bf, jnp.where(same_head, tiled, jnp.zeros_like(tiled)), NT)
        mean_square = mm((mixed * mixed).astype(BF16), mean_ones, NN)
        branch = mixed * lax.rsqrt(mean_square + EPSILON) * out_gain
        branch = branch * (gate_pre * sigmoid(gate_pre))
        return (stream + branch).astype(BF16), (values, key_end, ending)

    def advance(memory, carried):
        values, key_end, ending = carried
        spread_out = mm(values, key_end, TN)
        added = spread_out[0:HEAD]
        for h in range(1, heads):
            added = jnp.where(lane_head == h, spread_out[h * HEAD : (h + 1) * HEAD], added)
        return added if memory is None else memory * ending + added

    @pl.when(stage == 0)
    def _():
        def to_next(slot, parity, target):
            return pltpu.make_async_remote_copy(
                src_ref=res.at[slot, parity],
                dst_ref=buf.at[slot, parity, core, z],
                send_sem=send_sem.at[slot, parity],
                recv_sem=direct_sem.at[slot, z],
                device_id=at(1, target * 2 + 1 - parity),
                device_id_type=pl.DeviceIdType.MESH,
            )

        def forward(slot, parity):
            half = buf.at[slot, parity, other]
            return pltpu.make_async_remote_copy(
                src_ref=half,
                dst_ref=half,
                send_sem=forward_send,
                recv_sem=forward_sem.at[slot, parity],
                device_id=at(stage, partner),
                device_id_type=pl.DeviceIdType.MESH,
            )

        def pass_on(slot, parity):
            whole_wait(buf.at[slot, parity, other], direct_sem.at[slot, parity])
            forward(slot, parity).start()

        def sent(slot):
            for parity in range(2):
                whole_wait(buf.at[slot, parity, core], send_sem.at[slot, parity])

        def turn_of(slot, parity):
            @pl.when((slot > 0) & (parity == 0))
            def _():
                sent(slot - 1)

        def finish(slot, parity, part, product, inverse, memory):
            stream = buf[slot, parity, core, z].astype(F32)
            result, carried = mix(product, inverse, core, part, memory, stream)
            res[slot, parity] = result
            turn_of(slot, parity)
            own_first(lambda target: to_next(slot, parity, target).start())
            state[parity] = advance(memory, carried)

        pass_on(0, 0)

        def single(parity, carry):
            whole_wait(buf.at[0, parity, core], forward_sem.at[0, parity])
            scaled, inverse = gather(0, parity)
            product = mm(scaled, turned[core], NN)

            @pl.when(parity == 0)
            def _():
                pass_on(0, 1)

            @pl.when(parity == 1)
            def _():
                pass_on(1, 0)
                pass_on(1, 1)

            finish(0, parity, 0, product, inverse, None)
            return carry

        lax.fori_loop(0, 2, single, 0)

        def step(slot, carry):
            part = lax.rem(slot, parts)
            for parity in range(2):
                whole_wait(buf.at[slot, parity, core], forward_sem.at[slot, parity])
            both = [gather(slot, parity) for parity in range(2)]
            product = mm(jnp.concatenate([b[0] for b in both], axis=0), turned[core], NN)

            @pl.when(slot + 1 < slots)
            def _():
                pass_on(slot + 1, 0)
                pass_on(slot + 1, 1)

            for parity in range(2):
                memory = jnp.where(part == 0, 0.0, state[parity])
                own = product[parity * size : (parity + 1) * size]
                finish(slot, parity, part, own, both[parity][1], memory)
            return carry

        lax.fori_loop(1, slots, step, 0)

        whole_wait(buf.at[:, :, 0], forward_send)
        sent(slots - 1)

    @pl.when(stage != 0)
    def _():
        swap_tile(tiles - 1).start()
        swap_small(0).wait_recv()
        swap_small(1).wait_recv()
        spread(other)
        for group in range(groups):
            first, end = max(group * 3 - 1, 0), min(group * 3 + 2, tiles)
            lines = pl.ds(first * TILE, (end - first) * TILE)
            whole_wait(turned.at[other, lines], swap_recv.at[group])
            if group < 2:

                @pl.when(in_slot != 0)
                def _():
                    enter(group)

        parity = lax.rem(core + stage, 2)
        upper = z // ((chips + 1) // 2)

        def to_next(slot, target):
            return pltpu.make_async_remote_copy(
                src_ref=res.at[slot],
                dst_ref=buf.at[slot, parity, :, z],
                send_sem=send_sem.at[slot, 0],
                recv_sem=direct_sem.at[slot, z],
                device_id=at(lax.rem(stage + 1, stages), target * 2 + other),
                device_id_type=pl.DeviceIdType.MESH,
            )

        def owner(slot):
            part = lax.rem(slot, parts)
            return ((slot // parts) * 2 + parity) * spans + part // 2

        def place(slot):
            start = pl.multiple_of(lax.rem(slot, 2) * size, size)
            return out_ref.at[pl.ds(start, size)]

        def out_copy(slot, half):
            return pltpu.make_async_remote_copy(
                src_ref=res.at[slot, half],
                dst_ref=place(slot),
                send_sem=send_sem.at[slot, half],
                recv_sem=out_sem,
                device_id=at(owner(slot), z * 2 + half),
                device_id_type=pl.DeviceIdType.MESH,
            )

        def stays(slot, half):
            return (owner(slot) == stage) & (core == half)

        def step(slot, carry):
            part = lax.rem(slot, parts)
            squares, products = 0.0, [0.0, 0.0]
            for j in range(chips):
                k = upper * j + (1 - upper) * (chips - 1 - j)
                whole_wait(buf.at[slot, parity, :, k], direct_sem.at[slot, k])
                scaled, added = block(slot, parity, k)
                squares = squares + added
                span = pl.ds(pl.multiple_of(k * 2 * cols, 2 * cols), 2 * cols)
                for half in range(2):
                    products[half] = products[half] + mm(scaled, turned[half, span], NN)
            inverse = inverse_of(squares)
            kept = []
            for half in range(2):
                product = products[half]
                memory = jnp.where(part == 0, 0.0, state[half])
                stream = buf[slot, parity, half, z].astype(F32)
                result, carried = mix(product, inverse, half, part, memory, stream)
                res[slot, half] = result
                kept.append((memory, carried))

            @pl.when(stage != last)
            def _():
                own_first(lambda target: to_next(slot, target).start())

            for half in range(2):

                @pl.when((stage == last) & ~stays(slot, half))
                def _():
                    out_copy(slot, half).start()

                @pl.when((stage == last) & stays(slot, half))
                def _():
                    pltpu.make_async_copy(res.at[slot, half], place(slot), out_sem).start()

            for half in range(2):
                memory, carried = kept[half]
                state[half] = advance(memory, carried)
            return carry

        lax.fori_loop(0, slots, step, 0)

        def drain(slot, carry):
            @pl.when(stage != last)
            def _():
                whole_wait(buf.at[slot, 0], send_sem.at[slot, 0])

            for half in range(2):

                @pl.when((stage == last) & ~stays(slot, half))
                def _():
                    out_copy(slot, half).wait_send()

            return carry

        lax.fori_loop(0, slots, drain, 0)
        whole_wait(turned.at[core], swap_send.at[0])
        swap_small(0).wait_send()
        swap_small(1).wait_send()

    whole_wait(buf.at[0, 0], in_send)

    whole_wait(out_ref, out_sem)


def solution(mesh):
    stages = mesh.shape["pp"]
    lanes_axis = mesh.shape["tp"]
    chips = lanes_axis // 2

    def step(x, gain, wq, wf, wi, wg, low, spike, scale):
        rows, cols = x.shape
        width = gain.shape[1]
        positions = spike.shape[1]
        heads = cols // HEAD
        size = rows // 2
        parts = positions // size
        vmem = pl.BlockSpec(memory_space=pltpu.VMEM)
        hbm = pl.BlockSpec(memory_space=pl.ANY)
        dma = pltpu.SemaphoreType.DMA
        return pl.pallas_call(
            functools.partial(kernel, stages, lanes_axis),
            out_shape=jax.ShapeDtypeStruct((rows, cols), BF16),
            in_specs=[hbm] * 9,
            out_specs=vmem,
            scratch_shapes=[
                pltpu.VMEM((rows, cols), BF16),
                pltpu.VMEM((chips, 1, 2 * cols), F32),
                pltpu.VMEM(scale.shape, F32),
                pltpu.VMEM((2, 1, cols), F32),
                pltpu.VMEM((2, heads, positions), F32),
                pltpu.VMEM((4 * cols, width), BF16),
                pltpu.VMEM((2, width, 4 * cols), BF16),
                pltpu.VMEM((stages, 2, 2, chips, size, cols), BF16),
                pltpu.VMEM((stages, 2, size, cols), BF16),
                pltpu.VMEM((2, parts, size, cols), F32),
                pltpu.VMEM((2, HEAD, cols), F32),
                dma((5,)),
                dma,
                dma((3,)),
                dma((width // TILE // 3 + 3,)),
                dma,
                dma((stages, chips)),
                dma((stages, 2)),
                dma,
                dma((stages, 2)),
                dma,
            ],
            compiler_params=pltpu.CompilerParams(
                collective_id=0, has_side_effects=True, vmem_limit_bytes=GRANT
            ),
        )(
            *[
                pltpu.with_memory_space_constraint(v, pltpu.HBM)
                for v in (x, gain, wq, wf, wi, wg, low, spike.transpose(0, 2, 1), scale)
            ]
        )

    in_specs = (
        P("pp", "tp"),
        P("pp", None),
        P("pp", "tp", None),
        P("pp", "tp", None),
        P("pp", "tp", None),
        P("pp", "tp", None),
        P("pp", "tp"),
        P("pp", None, "tp"),
        P("pp", None),
    )
    return jax.shard_map(
        step, mesh=mesh, in_specs=in_specs, out_specs=P("pp", "tp"), check_vma=False
    )
```

```python
import functools

import jax
import jax.numpy as jnp
from jax import lax
from jax.experimental import pallas as pl
from jax.experimental.pallas import tpu as pltpu
from jax.sharding import PartitionSpec as P

HEAD = 64
TILE = 256
EPSILON = 1e-06
GRANT = 40 * 2**20
F32 = jnp.float32
BF16 = jnp.bfloat16
NT = (((1,), (1,)), ((), ()))
NN = (((1,), (0,)), ((), ()))
TN = (((0,), (0,)), ((), ()))


def mm(a, b, dims):
    return lax.dot_general(a, b, dims, preferred_element_type=F32)


def sigmoid(v):
    return 1.0 / (1.0 + jnp.exp(-v))


def at(stage, lane):
    return {"pp": stage, "tp": lane}


def kernel(
    stages,
    lanes_axis,
    x_ref,
    gain_ref,
    wq_ref,
    wf_ref,
    wi_ref,
    wg_ref,
    low_ref,
    spike_ref,
    scale_ref,
    out_ref,
    xv,
    gain_v,
    scale_v,
    lows,
    spike_raw,
    weights,
    turned,
    buf,
    res,
    spikes,
    state,
    load_sem,
    w_sem,
    swap_send,
    swap_recv,
    in_send,
    direct_sem,
    forward_sem,
    forward_send,
    send_sem,
    out_sem,
):
    rows, cols = xv.shape
    size = buf.shape[4]
    heads = cols // HEAD
    width = turned.shape[1]
    positions = spike_raw.shape[2]
    tiles = width // TILE
    groups = tiles // 3 + 1
    parts = positions // size
    spans = positions // rows
    chips = lanes_axis // 2
    slots = stages
    last = stages - 1
    stage = lax.axis_index("pp")
    lane = lax.axis_index("tp")
    core = lax.rem(lane, 2)
    other = 1 - core
    z = lane // 2
    partner = z * 2 + other

    barrier = pltpu.get_barrier_semaphore()

    def ready(to_stage, to_lane):
        pl.semaphore_signal(
            barrier,
            inc=1,
            device_id=at(to_stage, to_lane),
            device_id_type=pl.DeviceIdType.MESH,
        )

    ready(stage, partner)

    @pl.when(stage == 0)
    def _():
        for source in range(stages):
            for over in range(chips):
                ready(source, over * 2 + other)

    @pl.when(stage == 1)
    def _():
        for over in range(lanes_axis):
            ready(0, over)

    @pl.when(stage > 1)
    def _():
        for over in range(chips):
            ready(stage - 1, over * 2 + other)

    ready_from_last = [(last, z * 2 + c) for c in range(2)]
    for c in range(2):

        @pl.when((stage != last) | (core != c))
        def _():
            ready(*ready_from_last[c])

    onward = jnp.where(
        stage == 0,
        2 * chips,
        jnp.where(stage == last, 2 * stages - 1, chips),
    )
    greetings = 1 + chips + onward

    small = [
        pltpu.make_async_copy(scale_ref, scale_v, load_sem.at[2]),
        pltpu.make_async_copy(low_ref, lows.at[core], load_sem.at[3]),
        pltpu.make_async_copy(spike_ref.at[0], spike_raw.at[core], load_sem.at[4]),
    ]
    x_load = pltpu.make_async_copy(x_ref, xv, load_sem.at[0])
    x_load.start()
    for k in range(chips):
        pltpu.make_async_copy(
            gain_ref.at[:, k * 2 * cols : (k + 1) * 2 * cols], gain_v.at[k], load_sem.at[1]
        ).start()
    for load in small:
        load.start()
    for role, ref in enumerate((wq_ref, wf_ref, wi_ref, wg_ref)):
        pltpu.make_async_copy(
            ref.at[0], weights.at[pl.ds(role * cols, cols)], w_sem
        ).start()

    sequence = stage // spans
    in_parity = lax.rem(sequence, 2)
    in_slot = (sequence // 2) * parts + lax.rem(stage, spans) * 2

    def whole_wait(ref, sem):
        pltpu.make_async_copy(ref, ref, sem).wait()

    def farthest_first(send):
        for far in range(chips - 1, 0, -1):

            @pl.when(z + far < chips)
            def _():
                send(z + far)

            @pl.when(z - far >= 0)
            def _():
                send(z - far)

    def own_first(send):
        send(z)
        farthest_first(send)

    def to_first(target, half):
        return pltpu.make_async_remote_copy(
            src_ref=xv.at[pl.ds(half * size, size)],
            dst_ref=buf.at[in_slot + half, in_parity, core, z],
            send_sem=in_send,
            recv_sem=direct_sem.at[in_slot + half, in_parity],
            device_id=at(0, target * 2 + other),
            device_id_type=pl.DeviceIdType.MESH,
        )

    def enter(half):
        farthest_first(lambda target: to_first(target, half).start())
        to_first(z, half).start()

    def swap_small(which):
        src, dst = (
            (lows.at[core], lows.at[core])
            if which == 0
            else (spike_raw.at[core], spike_raw.at[core])
        )
        return pltpu.make_async_remote_copy(
            src_ref=src,
            dst_ref=dst,
            send_sem=swap_send.at[1 + which],
            recv_sem=swap_recv.at[groups + which],
            device_id=at(stage, partner),
            device_id_type=pl.DeviceIdType.MESH,
        )

    def swap_tile(k):
        tile = turned.at[core, pl.ds(pl.multiple_of(k * TILE, TILE), TILE)]
        return pltpu.make_async_remote_copy(
            src_ref=tile,
            dst_ref=tile,
            send_sem=swap_send.at[0],
            recv_sem=swap_recv.at[(k + 1) // 3],
            device_id=at(stage, partner),
            device_id_type=pl.DeviceIdType.MESH,
        )

    head_of_lane = lax.broadcasted_iota(jnp.int32, (size, cols), 1) // HEAD
    row = lax.broadcasted_iota(jnp.int32, (size, cols), 0)
    tall_row = lax.rem(lax.broadcasted_iota(jnp.int32, (heads * size, size), 0), size)
    tall_col = lax.broadcasted_iota(jnp.int32, (heads * size, size), 1)
    tall_mask = tall_row >= tall_col
    sq_row = lax.broadcasted_iota(jnp.int32, (cols, cols), 0) // HEAD
    sq_col = lax.broadcasted_iota(jnp.int32, (cols, cols), 1) // HEAD
    same_head = sq_row == sq_col
    lane_head = lax.broadcasted_iota(jnp.int32, (HEAD, cols), 1) // HEAD
    mean_ones = jnp.where(same_head, 1.0 / HEAD, 0.0).astype(BF16)

    def spread(half):
        for part in range(parts):
            piece = spike_raw[half, :, part * size : (part + 1) * size].T
            wide = jnp.zeros((size, cols), F32)
            for h in range(heads):
                wide = jnp.where(head_of_lane == h, piece[:, h : h + 1], wide)
            spikes[half, part] = jnp.exp(wide)

    x_load.wait()
    pl.semaphore_wait(barrier, greetings)

    @pl.when(in_slot == 0)
    def _():
        enter(0)

    for load in small:
        load.wait()
    whole_wait(gain_v, load_sem.at[1])

    @pl.when(stage != 0)
    def _():
        swap_small(0).start()
        swap_small(1).start()

    spread(core)
    whole_wait(weights, w_sem)

    def turn(k, carry):
        tile = pl.ds(pl.multiple_of(k * TILE, TILE), TILE)
        for role in range(4):
            turned[core, tile, role * cols : (role + 1) * cols] = weights[
                role * cols : (role + 1) * cols, tile
            ].T

        @pl.when((stage != 0) & (k > 0))
        def _():
            swap_tile(k - 1).start()

        return carry

    lax.fori_loop(0, width // TILE, turn, 0)

    @pl.when(in_slot == 0)
    def _():
        enter(1)

    def block(slot, parity, k):
        current = jnp.concatenate(
            [buf[slot, parity, c, k] for c in range(2)], axis=1
        ).astype(F32)
        squares = jnp.sum(current * current, axis=1, keepdims=True)
        return (current * gain_v[k]).astype(BF16), squares

    def gather(slot, parity):
        blocks = [block(slot, parity, k) for k in range(chips)]
        scaled = jnp.concatenate([b[0] for b in blocks], axis=1)
        return scaled, inverse_of(sum(b[1] for b in blocks))

    def inverse_of(squares):
        return lax.rsqrt(squares / width + EPSILON)

    out_gain = jnp.concatenate([scale_v[...]] * heads, axis=1)

    def mix(product, inverse, half, part, memory, stream):
        projected = product * inverse
        query_pre = projected[:, 0 * cols : 1 * cols]
        forget_pre = projected[:, 1 * cols : 2 * cols]
        values = projected[:, 2 * cols : 3 * cols].astype(BF16)
        gate_pre = projected[:, 3 * cols : 4 * cols]

        key_in = (1.0 - lows[half]) * sigmoid(-forget_pre)
        decay = (1.0 - key_in) * spikes[half, part]
        reach = 1
        while reach < size:
            decay = decay * jnp.where(row < reach, 1.0, pltpu.roll(decay, reach, 0))
            reach *= 2
        ending = decay[size - 1 : size, :]
        query_scaled = query_pre * sigmoid(query_pre) * decay
        key_grown = key_in / decay
        key_scaled = key_grown.astype(BF16)
        key_end = (key_grown * ending).astype(BF16)
        query_bf = query_scaled.astype(BF16)
        tall_query = jnp.concatenate(
            [jnp.where(head_of_lane == h, query_scaled, 0.0).astype(BF16) for h in range(heads)],
            axis=0,
        )
        scores = jnp.where(tall_mask, mm(tall_query, key_scaled, NT), 0.0).astype(BF16)
        tall_mixed = mm(scores, values, NN)
        mixed = tall_mixed[0:size]
        for h in range(1, heads):
            mixed = jnp.where(head_of_lane == h, tall_mixed[h * size : (h + 1) * size], mixed)
        if memory is not None:
            tiled = jnp.concatenate([memory.astype(BF16)] * heads, axis=0)
            mixed = mixed + mm(query_bf, jnp.where(same_head, tiled, jnp.zeros_like(tiled)), NT)
        mean_square = mm((mixed * mixed).astype(BF16), mean_ones, NN)
        branch = mixed * lax.rsqrt(mean_square + EPSILON) * out_gain
        branch = branch * (gate_pre * sigmoid(gate_pre))
        return (stream + branch).astype(BF16), (values, key_end, ending)

    def advance(memory, carried):
        values, key_end, ending = carried
        spread_out = mm(values, key_end, TN)
        added = spread_out[0:HEAD]
        for h in range(1, heads):
            added = jnp.where(lane_head == h, spread_out[h * HEAD : (h + 1) * HEAD], added)
        return added if memory is None else memory * ending + added

    @pl.when(stage == 0)
    def _():
        def to_next(slot, parity, target):
            return pltpu.make_async_remote_copy(
                src_ref=res.at[slot, parity],
                dst_ref=buf.at[slot, parity, core, z],
                send_sem=send_sem.at[slot, parity],
                recv_sem=direct_sem.at[slot, 0],
                device_id=at(1, target * 2 + 1 - parity),
                device_id_type=pl.DeviceIdType.MESH,
            )

        def forward(slot, parity):
            half = buf.at[slot, parity, other]
            return pltpu.make_async_remote_copy(
                src_ref=half,
                dst_ref=half,
                send_sem=forward_send,
                recv_sem=forward_sem.at[slot, parity],
                device_id=at(stage, partner),
                device_id_type=pl.DeviceIdType.MESH,
            )

        def pass_on(slot, parity):
            whole_wait(buf.at[slot, parity, other], direct_sem.at[slot, parity])
            forward(slot, parity).start()

        def sent(slot, parity):
            whole_wait(buf.at[slot, parity, core], send_sem.at[slot, parity])

        def turn_of(slot, parity):
            @pl.when(slot * 2 + parity > 0)
            def _():
                before = slot * 2 + parity - 1
                sent(before // 2, lax.rem(before, 2))

        def finish(slot, parity, part, product, inverse, memory):
            stream = buf[slot, parity, core, z].astype(F32)
            result, carried = mix(product, inverse, core, part, memory, stream)
            res[slot, parity] = result
            turn_of(slot, parity)
            own_first(lambda target: to_next(slot, parity, target).start())
            state[parity] = advance(memory, carried)

        pass_on(0, 0)

        def single(parity, carry):
            whole_wait(buf.at[0, parity, core], forward_sem.at[0, parity])
            scaled, inverse = gather(0, parity)
            product = mm(scaled, turned[core], NN)

            @pl.when(parity == 0)
            def _():
                pass_on(0, 1)

            @pl.when(parity == 1)
            def _():
                pass_on(1, 0)
                pass_on(1, 1)

            finish(0, parity, 0, product, inverse, None)
            return carry

        lax.fori_loop(0, 2, single, 0)

        def step(slot, carry):
            part = lax.rem(slot, parts)
            for parity in range(2):
                whole_wait(buf.at[slot, parity, core], forward_sem.at[slot, parity])
            both = [gather(slot, parity) for parity in range(2)]
            product = mm(jnp.concatenate([b[0] for b in both], axis=0), turned[core], NN)

            @pl.when(slot + 1 < slots)
            def _():
                pass_on(slot + 1, 0)
                pass_on(slot + 1, 1)

            for parity in range(2):
                memory = jnp.where(part == 0, 0.0, state[parity])
                own = product[parity * size : (parity + 1) * size]
                finish(slot, parity, part, own, both[parity][1], memory)
            return carry

        lax.fori_loop(1, slots, step, 0)

        whole_wait(buf.at[:, :, 0], forward_send)
        sent(slots - 1, 1)

    @pl.when(stage != 0)
    def _():
        swap_tile(tiles - 1).start()
        swap_small(0).wait_recv()
        swap_small(1).wait_recv()
        spread(other)
        for group in range(groups):
            first, end = max(group * 3 - 1, 0), min(group * 3 + 2, tiles)
            lines = pl.ds(first * TILE, (end - first) * TILE)
            whole_wait(turned.at[other, lines], swap_recv.at[group])
            if group < 2:

                @pl.when(in_slot != 0)
                def _():
                    enter(group)

        parity = lax.rem(core + stage, 2)

        def to_next(slot, target):
            return pltpu.make_async_remote_copy(
                src_ref=res.at[slot],
                dst_ref=buf.at[slot, parity, :, z],
                send_sem=send_sem.at[slot, 0],
                recv_sem=direct_sem.at[slot, 0],
                device_id=at(lax.rem(stage + 1, stages), target * 2 + other),
                device_id_type=pl.DeviceIdType.MESH,
            )

        def owner(slot):
            part = lax.rem(slot, parts)
            return ((slot // parts) * 2 + parity) * spans + part // 2

        def place(slot):
            start = pl.multiple_of(lax.rem(slot, 2) * size, size)
            return out_ref.at[pl.ds(start, size)]

        def out_copy(slot, half):
            return pltpu.make_async_remote_copy(
                src_ref=res.at[slot, half],
                dst_ref=place(slot),
                send_sem=send_sem.at[slot, half],
                recv_sem=out_sem,
                device_id=at(owner(slot), z * 2 + half),
                device_id_type=pl.DeviceIdType.MESH,
            )

        def stays(slot, half):
            return (owner(slot) == stage) & (core == half)

        def step(slot, carry):
            part = lax.rem(slot, parts)
            whole_wait(buf.at[slot, parity], direct_sem.at[slot, 0])
            scaled, inverse = gather(slot, parity)
            products = [mm(scaled, turned[half], NN) for half in range(2)]
            kept = []
            for half in range(2):
                product = products[half]
                memory = jnp.where(part == 0, 0.0, state[half])
                stream = buf[slot, parity, half, z].astype(F32)
                result, carried = mix(product, inverse, half, part, memory, stream)
                res[slot, half] = result
                kept.append((memory, carried))

            @pl.when(stage != last)
            def _():
                own_first(lambda target: to_next(slot, target).start())

            for half in range(2):

                @pl.when((stage == last) & ~stays(slot, half))
                def _():
                    out_copy(slot, half).start()

                @pl.when((stage == last) & stays(slot, half))
                def _():
                    pltpu.make_async_copy(res.at[slot, half], place(slot), out_sem).start()

            for half in range(2):
                memory, carried = kept[half]
                state[half] = advance(memory, carried)
            return carry

        lax.fori_loop(0, slots, step, 0)

        def drain(slot, carry):
            @pl.when(stage != last)
            def _():
                whole_wait(buf.at[slot, 0], send_sem.at[slot, 0])

            for half in range(2):

                @pl.when((stage == last) & ~stays(slot, half))
                def _():
                    out_copy(slot, half).wait_send()

            return carry

        lax.fori_loop(0, slots, drain, 0)
        whole_wait(turned.at[core], swap_send.at[0])
        swap_small(0).wait_send()
        swap_small(1).wait_send()

    whole_wait(buf.at[0, 0], in_send)

    whole_wait(out_ref, out_sem)


def solution(mesh):
    stages = mesh.shape["pp"]
    lanes_axis = mesh.shape["tp"]
    chips = lanes_axis // 2

    def step(x, gain, wq, wf, wi, wg, low, spike, scale):
        rows, cols = x.shape
        width = gain.shape[1]
        positions = spike.shape[1]
        heads = cols // HEAD
        size = rows // 2
        parts = positions // size
        vmem = pl.BlockSpec(memory_space=pltpu.VMEM)
        hbm = pl.BlockSpec(memory_space=pl.ANY)
        dma = pltpu.SemaphoreType.DMA
        return pl.pallas_call(
            functools.partial(kernel, stages, lanes_axis),
            out_shape=jax.ShapeDtypeStruct((rows, cols), BF16),
            in_specs=[hbm] * 9,
            out_specs=vmem,
            scratch_shapes=[
                pltpu.VMEM((rows, cols), BF16),
                pltpu.VMEM((chips, 1, 2 * cols), F32),
                pltpu.VMEM(scale.shape, F32),
                pltpu.VMEM((2, 1, cols), F32),
                pltpu.VMEM((2, heads, positions), F32),
                pltpu.VMEM((4 * cols, width), BF16),
                pltpu.VMEM((2, width, 4 * cols), BF16),
                pltpu.VMEM((stages, 2, 2, chips, size, cols), BF16),
                pltpu.VMEM((stages, 2, size, cols), BF16),
                pltpu.VMEM((2, parts, size, cols), F32),
                pltpu.VMEM((2, HEAD, cols), F32),
                dma((5,)),
                dma,
                dma((3,)),
                dma((width // TILE // 3 + 3,)),
                dma,
                dma((stages, 2)),
                dma((stages, 2)),
                dma,
                dma((stages, 2)),
                dma,
            ],
            compiler_params=pltpu.CompilerParams(
                collective_id=0, has_side_effects=True, vmem_limit_bytes=GRANT
            ),
        )(
            *[
                pltpu.with_memory_space_constraint(v, pltpu.HBM)
                for v in (x, gain, wq, wf, wi, wg, low, spike.transpose(0, 2, 1), scale)
            ]
        )

    in_specs = (
        P("pp", "tp"),
        P("pp", None),
        P("pp", "tp", None),
        P("pp", "tp", None),
        P("pp", "tp", None),
        P("pp", "tp", None),
        P("pp", "tp"),
        P("pp", None, "tp"),
        P("pp", None),
    )
    return jax.shard_map(
        step, mesh=mesh, in_specs=in_specs, out_specs=P("pp", "tp"), check_vma=False
    )
```

```python
import functools

import jax
import jax.numpy as jnp
from jax import lax
from jax.experimental import pallas as pl
from jax.experimental.pallas import tpu as pltpu
from jax.sharding import PartitionSpec as P

HEAD = 64
TILE = 256
EPSILON = 1e-06
GRANT = 40 * 2**20
F32 = jnp.float32
BF16 = jnp.bfloat16
NT = (((1,), (1,)), ((), ()))
NN = (((1,), (0,)), ((), ()))
TN = (((0,), (0,)), ((), ()))


def mm(a, b, dims):
    return lax.dot_general(a, b, dims, preferred_element_type=F32)


def sigmoid(v):
    return 1.0 / (1.0 + jnp.exp(-v))


def at(stage, lane):
    return {"pp": stage, "tp": lane}


def kernel(
    stages,
    lanes_axis,
    x_ref,
    gain_ref,
    wq_ref,
    wf_ref,
    wi_ref,
    wg_ref,
    low_ref,
    spike_ref,
    scale_ref,
    out_ref,
    xv,
    gain_v,
    scale_v,
    lows,
    spike_raw,
    weights,
    turned,
    buf,
    res,
    spikes,
    state,
    load_sem,
    w_sem,
    swap_send,
    swap_recv,
    in_send,
    direct_sem,
    forward_sem,
    forward_send,
    send_sem,
    out_sem,
):
    rows, cols = xv.shape
    size = buf.shape[4]
    heads = cols // HEAD
    width = turned.shape[1]
    positions = spike_raw.shape[2]
    tiles = width // TILE
    groups = tiles // 3 + 1
    parts = positions // size
    spans = positions // rows
    chips = lanes_axis // 2
    slots = stages
    last = stages - 1
    stage = lax.axis_index("pp")
    lane = lax.axis_index("tp")
    core = lax.rem(lane, 2)
    other = 1 - core
    z = lane // 2
    partner = z * 2 + other

    barrier = pltpu.get_barrier_semaphore()

    def ready(to_stage, to_lane):
        pl.semaphore_signal(
            barrier,
            inc=1,
            device_id=at(to_stage, to_lane),
            device_id_type=pl.DeviceIdType.MESH,
        )

    ready(stage, partner)

    @pl.when(stage == 0)
    def _():
        for source in range(stages):
            for over in range(chips):
                ready(source, over * 2 + other)

    @pl.when(stage == 1)
    def _():
        for over in range(lanes_axis):
            ready(0, over)

    @pl.when(stage > 1)
    def _():
        for over in range(chips):
            ready(stage - 1, over * 2 + other)

    ready_from_last = [(last, z * 2 + c) for c in range(2)]
    for c in range(2):

        @pl.when((stage != last) | (core != c))
        def _():
            ready(*ready_from_last[c])

    onward = jnp.where(
        stage == 0,
        2 * chips,
        jnp.where(stage == last, 2 * stages - 1, chips),
    )
    greetings = 1 + chips + onward

    small = [
        pltpu.make_async_copy(scale_ref, scale_v, load_sem.at[2]),
        pltpu.make_async_copy(low_ref, lows.at[core], load_sem.at[3]),
        pltpu.make_async_copy(spike_ref.at[0], spike_raw.at[core], load_sem.at[4]),
    ]
    x_load = pltpu.make_async_copy(x_ref, xv, load_sem.at[0])
    x_load.start()
    for k in range(chips):
        pltpu.make_async_copy(
            gain_ref.at[:, k * 2 * cols : (k + 1) * 2 * cols], gain_v.at[k], load_sem.at[1]
        ).start()
    for load in small:
        load.start()
    for role, ref in enumerate((wf_ref, wq_ref, wi_ref, wg_ref)):
        pltpu.make_async_copy(
            ref.at[0], weights.at[pl.ds(role * cols, cols)], w_sem
        ).start()

    sequence = stage // spans
    in_parity = lax.rem(sequence, 2)
    in_slot = (sequence // 2) * parts + lax.rem(stage, spans) * 2

    def whole_wait(ref, sem):
        pltpu.make_async_copy(ref, ref, sem).wait()

    def farthest_first(send):
        for far in range(chips - 1, 0, -1):

            @pl.when(z + far < chips)
            def _():
                send(z + far)

            @pl.when(z - far >= 0)
            def _():
                send(z - far)

    def own_first(send):
        send(z)
        farthest_first(send)

    def to_first(target, half):
        return pltpu.make_async_remote_copy(
            src_ref=xv.at[pl.ds(half * size, size)],
            dst_ref=buf.at[in_slot + half, in_parity, core, z],
            send_sem=in_send,
            recv_sem=direct_sem.at[in_slot + half, in_parity],
            device_id=at(0, target * 2 + other),
            device_id_type=pl.DeviceIdType.MESH,
        )

    def enter(half):
        farthest_first(lambda target: to_first(target, half).start())
        to_first(z, half).start()

    def swap_small(which):
        src, dst = (
            (lows.at[core], lows.at[core])
            if which == 0
            else (spike_raw.at[core], spike_raw.at[core])
        )
        return pltpu.make_async_remote_copy(
            src_ref=src,
            dst_ref=dst,
            send_sem=swap_send.at[1 + which],
            recv_sem=swap_recv.at[groups + which],
            device_id=at(stage, partner),
            device_id_type=pl.DeviceIdType.MESH,
        )

    def swap_tile(k):
        tile = turned.at[core, pl.ds(pl.multiple_of(k * TILE, TILE), TILE)]
        return pltpu.make_async_remote_copy(
            src_ref=tile,
            dst_ref=tile,
            send_sem=swap_send.at[0],
            recv_sem=swap_recv.at[(k + 1) // 3],
            device_id=at(stage, partner),
            device_id_type=pl.DeviceIdType.MESH,
        )

    head_of_lane = lax.broadcasted_iota(jnp.int32, (size, cols), 1) // HEAD
    row = lax.broadcasted_iota(jnp.int32, (size, cols), 0)
    tall_row = lax.rem(lax.broadcasted_iota(jnp.int32, (heads * size, size), 0), size)
    tall_col = lax.broadcasted_iota(jnp.int32, (heads * size, size), 1)
    tall_mask = tall_row >= tall_col
    sq_row = lax.broadcasted_iota(jnp.int32, (cols, cols), 0) // HEAD
    sq_col = lax.broadcasted_iota(jnp.int32, (cols, cols), 1) // HEAD
    same_head = sq_row == sq_col
    lane_head = lax.broadcasted_iota(jnp.int32, (HEAD, cols), 1) // HEAD
    mean_ones = jnp.where(same_head, 1.0 / HEAD, 0.0).astype(BF16)

    def spread(half):
        for part in range(parts):
            piece = spike_raw[half, :, part * size : (part + 1) * size].T
            wide = jnp.zeros((size, cols), F32)
            for h in range(heads):
                wide = jnp.where(head_of_lane == h, piece[:, h : h + 1], wide)
            spikes[half, part] = jnp.exp(wide)

    x_load.wait()
    pl.semaphore_wait(barrier, greetings)

    @pl.when(in_slot == 0)
    def _():
        enter(0)

    for load in small:
        load.wait()
    whole_wait(gain_v, load_sem.at[1])

    @pl.when(stage != 0)
    def _():
        swap_small(0).start()
        swap_small(1).start()

    spread(core)
    whole_wait(weights, w_sem)

    def turn(k, carry):
        tile = pl.ds(pl.multiple_of(k * TILE, TILE), TILE)
        for role in range(4):
            turned[core, tile, role * cols : (role + 1) * cols] = weights[
                role * cols : (role + 1) * cols, tile
            ].T

        @pl.when((stage != 0) & (k > 0))
        def _():
            swap_tile(k - 1).start()

        return carry

    lax.fori_loop(0, width // TILE, turn, 0)

    @pl.when(in_slot == 0)
    def _():
        enter(1)

    def block(slot, parity, k):
        current = jnp.concatenate(
            [buf[slot, parity, c, k] for c in range(2)], axis=1
        ).astype(F32)
        squares = jnp.sum(current * current, axis=1, keepdims=True)
        return (current * gain_v[k]).astype(BF16), squares

    def gather(slot, parity):
        blocks = [block(slot, parity, k) for k in range(chips)]
        scaled = jnp.concatenate([b[0] for b in blocks], axis=1)
        return scaled, inverse_of(sum(b[1] for b in blocks))

    def inverse_of(squares):
        return lax.rsqrt(squares / width + EPSILON)

    out_gain = jnp.concatenate([scale_v[...]] * heads, axis=1)

    def mix(product, inverse, half, part, memory, stream):
        projected = product * inverse
        forget_pre = projected[:, 0 * cols : 1 * cols]
        query_pre = projected[:, 1 * cols : 2 * cols]
        values = projected[:, 2 * cols : 3 * cols].astype(BF16)
        gate_pre = projected[:, 3 * cols : 4 * cols]

        key_in = (1.0 - lows[half]) * sigmoid(-forget_pre)
        decay = (1.0 - key_in) * spikes[half, part]
        reach = 1
        while reach < size:
            decay = decay * jnp.where(row < reach, 1.0, pltpu.roll(decay, reach, 0))
            reach *= 2
        ending = decay[size - 1 : size, :]
        query_scaled = query_pre * sigmoid(query_pre) * decay
        key_grown = key_in / decay
        key_scaled = key_grown.astype(BF16)
        key_end = (key_grown * ending).astype(BF16)
        query_bf = query_scaled.astype(BF16)
        tall_query = jnp.concatenate(
            [jnp.where(head_of_lane == h, query_scaled, 0.0).astype(BF16) for h in range(heads)],
            axis=0,
        )
        scores = jnp.where(tall_mask, mm(tall_query, key_scaled, NT), 0.0).astype(BF16)
        tall_mixed = mm(scores, values, NN)
        mixed = tall_mixed[0:size]
        for h in range(1, heads):
            mixed = jnp.where(head_of_lane == h, tall_mixed[h * size : (h + 1) * size], mixed)
        if memory is not None:
            tiled = jnp.concatenate([memory.astype(BF16)] * heads, axis=0)
            mixed = mixed + mm(query_bf, jnp.where(same_head, tiled, jnp.zeros_like(tiled)), NT)
        mean_square = mm((mixed * mixed).astype(BF16), mean_ones, NN)
        branch = mixed * lax.rsqrt(mean_square + EPSILON) * out_gain
        branch = branch * (gate_pre * sigmoid(gate_pre))
        return (stream + branch).astype(BF16), (values, key_end, ending)

    def advance(memory, carried):
        values, key_end, ending = carried
        spread_out = mm(values, key_end, TN)
        added = spread_out[0:HEAD]
        for h in range(1, heads):
            added = jnp.where(lane_head == h, spread_out[h * HEAD : (h + 1) * HEAD], added)
        return added if memory is None else memory * ending + added

    @pl.when(stage == 0)
    def _():
        def to_next(slot, parity, target):
            return pltpu.make_async_remote_copy(
                src_ref=res.at[slot, parity],
                dst_ref=buf.at[slot, parity, core, z],
                send_sem=send_sem.at[slot, parity],
                recv_sem=direct_sem.at[slot, 0],
                device_id=at(1, target * 2 + 1 - parity),
                device_id_type=pl.DeviceIdType.MESH,
            )

        def forward(slot, parity):
            half = buf.at[slot, parity, other]
            return pltpu.make_async_remote_copy(
                src_ref=half,
                dst_ref=half,
                send_sem=forward_send,
                recv_sem=forward_sem.at[slot, parity],
                device_id=at(stage, partner),
                device_id_type=pl.DeviceIdType.MESH,
            )

        def pass_on(slot, parity):
            whole_wait(buf.at[slot, parity, other], direct_sem.at[slot, parity])
            forward(slot, parity).start()

        def sent(slot, parity):
            whole_wait(buf.at[slot, parity, core], send_sem.at[slot, parity])

        def turn_of(slot, parity):
            @pl.when(slot * 2 + parity > 0)
            def _():
                before = slot * 2 + parity - 1
                sent(before // 2, lax.rem(before, 2))

        def finish(slot, parity, part, product, inverse, memory):
            stream = buf[slot, parity, core, z].astype(F32)
            result, carried = mix(product, inverse, core, part, memory, stream)
            res[slot, parity] = result
            turn_of(slot, parity)
            own_first(lambda target: to_next(slot, parity, target).start())
            state[parity] = advance(memory, carried)

        pass_on(0, 0)

        def single(parity, carry):
            whole_wait(buf.at[0, parity, core], forward_sem.at[0, parity])
            scaled, inverse = gather(0, parity)
            product = mm(scaled, turned[core], NN)

            @pl.when(parity == 0)
            def _():
                pass_on(0, 1)

            @pl.when(parity == 1)
            def _():
                pass_on(1, 0)
                pass_on(1, 1)

            finish(0, parity, 0, product, inverse, None)
            return carry

        lax.fori_loop(0, 2, single, 0)

        def step(slot, carry):
            part = lax.rem(slot, parts)
            for parity in range(2):
                whole_wait(buf.at[slot, parity, core], forward_sem.at[slot, parity])
            both = [gather(slot, parity) for parity in range(2)]
            product = mm(jnp.concatenate([b[0] for b in both], axis=0), turned[core], NN)

            @pl.when(slot + 1 < slots)
            def _():
                pass_on(slot + 1, 0)
                pass_on(slot + 1, 1)

            for parity in range(2):
                memory = jnp.where(part == 0, 0.0, state[parity])
                own = product[parity * size : (parity + 1) * size]
                finish(slot, parity, part, own, both[parity][1], memory)
            return carry

        lax.fori_loop(1, slots, step, 0)

        whole_wait(buf.at[:, :, 0], forward_send)
        sent(slots - 1, 1)

    @pl.when(stage != 0)
    def _():
        swap_tile(tiles - 1).start()
        swap_small(0).wait_recv()
        swap_small(1).wait_recv()
        spread(other)
        for group in range(groups):
            first, end = max(group * 3 - 1, 0), min(group * 3 + 2, tiles)
            lines = pl.ds(first * TILE, (end - first) * TILE)
            whole_wait(turned.at[other, lines], swap_recv.at[group])
            if group < 2:

                @pl.when(in_slot != 0)
                def _():
                    enter(group)

        parity = lax.rem(core + stage, 2)

        def to_next(slot, target):
            return pltpu.make_async_remote_copy(
                src_ref=res.at[slot],
                dst_ref=buf.at[slot, parity, :, z],
                send_sem=send_sem.at[slot, 0],
                recv_sem=direct_sem.at[slot, 0],
                device_id=at(lax.rem(stage + 1, stages), target * 2 + other),
                device_id_type=pl.DeviceIdType.MESH,
            )

        def owner(slot):
            part = lax.rem(slot, parts)
            return ((slot // parts) * 2 + parity) * spans + part // 2

        def place(slot):
            start = pl.multiple_of(lax.rem(slot, 2) * size, size)
            return out_ref.at[pl.ds(start, size)]

        def out_copy(slot, half):
            return pltpu.make_async_remote_copy(
                src_ref=res.at[slot, half],
                dst_ref=place(slot),
                send_sem=send_sem.at[slot, half],
                recv_sem=out_sem,
                device_id=at(owner(slot), z * 2 + half),
                device_id_type=pl.DeviceIdType.MESH,
            )

        def stays(slot, half):
            return (owner(slot) == stage) & (core == half)

        def step(slot, carry):
            part = lax.rem(slot, parts)
            whole_wait(buf.at[slot, parity], direct_sem.at[slot, 0])
            scaled, inverse = gather(slot, parity)
            products = [mm(scaled, turned[half], NN) for half in range(2)]
            kept = []
            for half in range(2):
                product = products[half]
                memory = jnp.where(part == 0, 0.0, state[half])
                stream = buf[slot, parity, half, z].astype(F32)
                result, carried = mix(product, inverse, half, part, memory, stream)
                res[slot, half] = result
                kept.append((memory, carried))

            @pl.when(stage != last)
            def _():
                own_first(lambda target: to_next(slot, target).start())

            for half in range(2):

                @pl.when((stage == last) & ~stays(slot, half))
                def _():
                    out_copy(slot, half).start()

                @pl.when((stage == last) & stays(slot, half))
                def _():
                    pltpu.make_async_copy(res.at[slot, half], place(slot), out_sem).start()

            for half in range(2):
                memory, carried = kept[half]
                state[half] = advance(memory, carried)
            return carry

        lax.fori_loop(0, slots, step, 0)

        def drain(slot, carry):
            @pl.when(stage != last)
            def _():
                whole_wait(buf.at[slot, 0], send_sem.at[slot, 0])

            for half in range(2):

                @pl.when((stage == last) & ~stays(slot, half))
                def _():
                    out_copy(slot, half).wait_send()

            return carry

        lax.fori_loop(0, slots, drain, 0)
        whole_wait(turned.at[core], swap_send.at[0])
        swap_small(0).wait_send()
        swap_small(1).wait_send()

    whole_wait(buf.at[0, 0], in_send)

    whole_wait(out_ref, out_sem)


def solution(mesh):
    stages = mesh.shape["pp"]
    lanes_axis = mesh.shape["tp"]
    chips = lanes_axis // 2

    def step(x, gain, wq, wf, wi, wg, low, spike, scale):
        rows, cols = x.shape
        width = gain.shape[1]
        positions = spike.shape[1]
        heads = cols // HEAD
        size = rows // 2
        parts = positions // size
        vmem = pl.BlockSpec(memory_space=pltpu.VMEM)
        hbm = pl.BlockSpec(memory_space=pl.ANY)
        dma = pltpu.SemaphoreType.DMA
        return pl.pallas_call(
            functools.partial(kernel, stages, lanes_axis),
            out_shape=jax.ShapeDtypeStruct((rows, cols), BF16),
            in_specs=[hbm] * 9,
            out_specs=vmem,
            scratch_shapes=[
                pltpu.VMEM((rows, cols), BF16),
                pltpu.VMEM((chips, 1, 2 * cols), F32),
                pltpu.VMEM(scale.shape, F32),
                pltpu.VMEM((2, 1, cols), F32),
                pltpu.VMEM((2, heads, positions), F32),
                pltpu.VMEM((4 * cols, width), BF16),
                pltpu.VMEM((2, width, 4 * cols), BF16),
                pltpu.VMEM((stages, 2, 2, chips, size, cols), BF16),
                pltpu.VMEM((stages, 2, size, cols), BF16),
                pltpu.VMEM((2, parts, size, cols), F32),
                pltpu.VMEM((2, HEAD, cols), F32),
                dma((5,)),
                dma,
                dma((3,)),
                dma((width // TILE // 3 + 3,)),
                dma,
                dma((stages, 2)),
                dma((stages, 2)),
                dma,
                dma((stages, 2)),
                dma,
            ],
            compiler_params=pltpu.CompilerParams(
                collective_id=0, has_side_effects=True, vmem_limit_bytes=GRANT
            ),
        )(
            *[
                pltpu.with_memory_space_constraint(v, pltpu.HBM)
                for v in (x, gain, wq, wf, wi, wg, low, spike.transpose(0, 2, 1), scale)
            ]
        )

    in_specs = (
        P("pp", "tp"),
        P("pp", None),
        P("pp", "tp", None),
        P("pp", "tp", None),
        P("pp", "tp", None),
        P("pp", "tp", None),
        P("pp", "tp"),
        P("pp", None, "tp"),
        P("pp", None),
    )
    return jax.shard_map(
        step, mesh=mesh, in_specs=in_specs, out_specs=P("pp", "tp"), check_vma=False
    )
```
